128 devices in a mesh: ep: 64 (over z, y, x), tp: 2 (over core).
Axes of the slice: x: 4, y: 4, z: 4, core: 2. Of those that a mesh axis runs over, the one named last changes fastest.
Arguments:
- inputs: bfloat16 [1024, 2048], P('ep'), may hold values from -6 to 6
- positions: int32 [1024], P('ep'), may hold values from 1024 to 8191
- ret_state: float32 [1024, 12, 128, 128], P('ep', 'tp'), may hold values from -4 to 4
- norm_mix: bfloat16 [2048], replicated, may hold values from 0.099609375 to 1.8984375
- w_query: bfloat16 [2048, 1536], P('ep', 'tp'), may hold values from -0.375 to 0.375
- w_key: bfloat16 [2048, 1536], P('ep', 'tp'), may hold values from -0.375 to 0.375
- w_value: bfloat16 [2048, 1536], P('ep', 'tp'), may hold values from -0.375 to 0.375
- w_gate_in: bfloat16 [2048, 1536], P('ep', 'tp'), may hold values from -0.375 to 0.375
- head_gain: bfloat16 [1536], P('tp'), may hold values from 0.099609375 to 1.8984375
- w_out: bfloat16 [1536, 2048], P('tp', 'ep'), may hold values from -0.15625 to 0.15625
- norm_ffn: bfloat16 [2048], replicated, may hold values from 0.099609375 to 1.8984375
- route_ids: int32 [1024, 4], P('ep'), may hold values from 0 to 63, all different within a row; in each aligned block of 16 rows (0 to 15, 16 to 31, ...) at most 2 rows name the same one
- route_weight: bfloat16 [1024, 4], P('ep'), may hold values from 0.19921875 to 1
- exp_gate: bfloat16 [64, 2048, 1024], P('ep', None, 'tp'), may hold values from -0.125 to 0.125
- exp_up: bfloat16 [64, 2048, 1024], P('ep', None, 'tp'), may hold values from -0.125 to 0.125
- exp_down: bfloat16 [64, 1024, 2048], P('ep', 'tp'), may hold values from -0.1875 to 0.1875
- dense_gate: bfloat16 [2048, 4096], P(None, ('ep', 'tp')), may hold values from -0.125 to 0.125
- dense_up: bfloat16 [2048, 4096], P(None, ('ep', 'tp')), may hold values from -0.125 to 0.125
- dense_down: bfloat16 [4096, 2048], P(('ep', 'tp')), may hold values from -0.375 to 0.375
- branch_gate: bfloat16 [2048], replicated, may hold values from -0.125 to 0.125
Outputs:
- layer_out: bfloat16 [1024, 2048], P('ep')
- new_state: float32 [1024, 12, 128, 128], P('ep', 'tp')
The draws below stay inside these ranges and needn't reach their ends.
Inputs may be any that keep to these rules, and one draw needn't show every extreme that they name: `route_ids`: each row names 4 different experts. Among the rows of one index of ep no expert is named more than 2 times, a bound that some block reaches.
All inputs are finite; a program needn't handle non-finite values.
Results may differ from the reference program's by a relative error of at most 0.015.
Values may be sent and summed in bfloat16 or wider, within the bound.
No kernel may reach another device: no remote copies, remote signals or barrier semaphores. Data moves between devices by JAX's collectives and lax.ppermute only.
A program may use at most 128 MiB of HBM per device.

```python
import math
from functools import reduce
import jax
import jax.numpy as jnp
import numpy as np
from jax import lax

D = 2048
HEADS = 12
HEAD_DIM = 128
EXP_FF = 1024
DENSE_FF = 4096
TOP_K = 4
SEQ_DEV = 16
RET_WIDTH = 1536
EXPERTS = 64
TOKENS = 1024
CAP = 2
N_EP = 64
N_TP = 2


def place_ends(drawn, stream_key, smallest, top_value):
    index_at = [jax.random.randint(jax.random.fold_in(stream_key, axis), (), 0, length) for axis, length in enumerate(drawn.shape)]
    longest = drawn.shape.index(max(drawn.shape))
    next_to = index_at[:longest] + [(index_at[longest] + 1) % drawn.shape[longest]] + index_at[longest + 1:]
    return drawn.at[tuple(index_at)].set(smallest).at[tuple(next_to)].set(top_value)


def raised(values, own_key, source, target, blocks, factor):
    def block_of(position):
        return (jnp.arange(values.shape[position]) // (values.shape[position] // blocks)).reshape((-1,) + (1,) * (values.ndim - 1 - position))

    first = jax.random.permutation(own_key, blocks)[block_of(target)]
    far = (block_of(target) + blocks // 2) % blocks
    return jnp.where((block_of(source) == first) | (block_of(source) == far), factor * values, values)


def block_scale(key, shape, shards, smallest, top_value):
    def one(axis_at, parts):
        draws = jax.random.uniform(jax.random.fold_in(jax.random.fold_in(key, 6), axis_at), (parts,), jnp.float32, smallest / len(shards), top_value / len(shards))
        return jnp.repeat(jnp.exp(draws), shape[axis_at] // parts).reshape((-1,) + (1,) * (len(shape) - axis_at - 1))

    loudness = one(*shards[0])
    for cut in shards[1:]:
        loudness = loudness * one(*cut)
    return loudness


def deal_out(rng, own, number, rows, amount, top, reach, lean):
    order = jax.random.permutation(rng, amount)
    heavy_load, ordinary = load_shares(amount, rows * top, reach, lean, True), load_shares(amount, rows * top, reach, lean, False)
    places = jnp.arange(amount)

    def named(lengths, turn):
        used = int((lengths > 0).sum())
        fixed = max(1, used // 4)
        moved = fixed + (places - fixed + turn * (used - fixed)) % max(1, amount - fixed)
        return jnp.zeros((amount,), jnp.int32).at[order[jnp.where(places < fixed, places, moved)]].set(jnp.asarray(lengths, jnp.int32))

    lengths = jnp.where(number % 4 == 0, named(heavy_load, number // 4), named(ordinary, number - number // 4 - 1))
    mixed = jax.random.permutation(jax.random.fold_in(own, 3), amount)
    giver, receiver = mixed[0:amount // 2 * 2:2], mixed[1:amount // 2 * 2:2]
    margin = jnp.minimum(lengths[giver] - 1, reach - lengths[receiver]) // 2
    margin = jnp.where((giver == order[0]) | (receiver == order[0]) | (lengths[receiver] == 0), 0, jnp.maximum(margin, 0))
    moved = jax.random.randint(jax.random.fold_in(own, 4), (amount // 2,), 0, 1 << 20) % (margin + 1)
    lengths = lengths.at[giver].add(-moved).at[receiver].add(moved)
    items = jnp.searchsorted(jnp.cumsum(lengths), jnp.arange(rows * top), side="right").astype(jnp.int32)
    grid = items.reshape(top, rows).T
    grid = grid[jax.random.permutation(jax.random.fold_in(own, 1), rows)]
    turn = jax.random.randint(jax.random.fold_in(own, 2), (rows, 1), 0, top)
    return jnp.take_along_axis(grid, (jnp.arange(top)[None, :] + turn) % top, axis=1)


def load_shares(amount, total, bound, slope, full):
    portions = [(1 << 20) // math.isqrt(standing ** slope) + 1 for standing in range(1, amount + 1)]
    largest = bound if full else min(bound, max(-(-total // amount), total * portions[0] // sum(portions)))
    least = 1 if total - largest >= amount - 1 else 0
    given, rest = [largest] + [least] * (amount - 1), total - largest - least * (amount - 1)
    while rest > 0:
        candidates = [i for i in range(1, amount) if given[i] < largest] or [i for i in range(1, amount) if given[i] < bound]
        pool, budget = sum([portions[i] for i in candidates]), rest
        for i in candidates:
            addition = min(bound - given[i], max(1, budget * portions[i] // pool), rest)
            given[i] = given[i] + addition
            rest = rest - addition
    return np.array(given)


def scatter_about(stream_key, dims, scale, bound, pieces=(), kind=jnp.bfloat16):
    drawn = jax.random.normal(stream_key, dims, jnp.float32) * scale
    if len(pieces) > 0:
        drawn = block_scale(stream_key, dims, pieces, -0.22, 0.18) * drawn
    return jnp.clip(drawn, min=-bound, max=bound).astype(kind)


def gaussian_with(key, dims, deviation, reach, shards, heavy, kind=jnp.bfloat16):
    values = deviation * jax.random.normal(key, dims, jnp.float32)
    if shards:
        values = values * block_scale(key, dims, shards, -0.22, 0.18)
    return jnp.clip(raised(values, jax.random.fold_in(key, 3), *heavy), -reach, reach).astype(kind)


def setup_inputs(seed: int = 0) -> dict:
    keys = jax.random.split(jax.random.key(seed), 21)
    inputs = scatter_about(keys[0], (TOKENS, D), 1.0, 6.0, ((0, 64),))
    positions = place_ends(jax.random.randint(keys[1], (TOKENS,), 1024, 8192), jax.random.fold_in(keys[1], 1), 1024, 8191).astype(jnp.int32)
    ret_state = scatter_about(keys[2], (TOKENS, HEADS, HEAD_DIM, HEAD_DIM), 0.25, 4.0, ((0, 64), (1, 2)), jnp.float32)
    norm_mix = jnp.clip(1.0 + 0.18 * jax.random.normal(keys[3], (D,), jnp.float32), 0.099609375, 1.8984375).astype(jnp.bfloat16)
    w_query = gaussian_with(keys[4], (D, RET_WIDTH), D ** -0.5, 0.375, ((0, 64), (1, 2)), (0, 1, 64, 4.0))
    w_key = gaussian_with(keys[5], (D, RET_WIDTH), D ** -0.5, 0.375, ((0, 64), (1, 2)), (0, 1, 64, 4.0))
    w_value = gaussian_with(keys[6], (D, RET_WIDTH), D ** -0.5, 0.375, ((0, 64), (1, 2)), (0, 1, 64, 4.0))
    w_gate_in = gaussian_with(keys[7], (D, RET_WIDTH), D ** -0.5, 0.375, ((0, 64), (1, 2)), (0, 1, 64, 4.0))
    head_gain = jnp.clip(1.0 + 0.18 * jax.random.normal(keys[8], (RET_WIDTH,), jnp.float32), 0.099609375, 1.8984375).astype(jnp.bfloat16)
    w_out = scatter_about(keys[9], (RET_WIDTH, D), RET_WIDTH ** -0.5, 0.15625, ((0, 2), (1, 64)))
    norm_ffn = jnp.clip(1.0 + 0.18 * jax.random.normal(keys[10], (D,), jnp.float32), 0.099609375, 1.8984375).astype(jnp.bfloat16)
    route_ids_keys = jax.random.split(jax.random.fold_in(keys[11], 1), TOKENS // SEQ_DEV)
    route_ids_turns = jax.random.permutation(jax.random.fold_in(keys[11], 3), TOKENS // SEQ_DEV)
    route_ids = jax.vmap(lambda own, number: deal_out(jax.random.fold_in(keys[11], 2), own, number, SEQ_DEV, EXPERTS, TOP_K, CAP, 2))(route_ids_keys, route_ids_turns).reshape((TOKENS, TOP_K))
    route_weight = jnp.clip(jnp.exp(math.log(1.0) - 1.6133518 * jax.random.uniform(keys[12], (TOKENS, TOP_K), jnp.float32) ** block_scale(keys[12], (TOKENS, TOP_K), ((0, 64),), -0.2, 0.2)), 0.19921875, 1.0).astype(jnp.bfloat16)
    exp_gate = scatter_about(keys[13], (EXPERTS, D, EXP_FF), D ** -0.5, 0.125, ((0, 64), (2, 2)))
    exp_up = scatter_about(keys[14], (EXPERTS, D, EXP_FF), D ** -0.5, 0.125, ((0, 64), (2, 2)))
    exp_down = scatter_about(keys[15], (EXPERTS, EXP_FF, D), EXP_FF ** -0.5, 0.1875, ((0, 64), (1, 2)))
    dense_gate = scatter_about(keys[16], (D, DENSE_FF), D ** -0.5, 0.125, ((1, 128),))
    dense_up = scatter_about(keys[17], (D, DENSE_FF), D ** -0.5, 0.125, ((1, 128),))
    dense_down = gaussian_with(keys[18], (DENSE_FF, D), DENSE_FF ** -0.5, 0.375, ((0, 128),), (0, 1, 128, 5.5))
    branch_gate = scatter_about(keys[19], (D,), D ** -0.5, 0.125)
    return {"inputs": inputs, "positions": positions, "ret_state": ret_state, "norm_mix": norm_mix, "w_query": w_query, "w_key": w_key, "w_value": w_value, "w_gate_in": w_gate_in, "head_gain": head_gain, "w_out": w_out, "norm_ffn": norm_ffn, "route_ids": route_ids, "route_weight": route_weight, "exp_gate": exp_gate, "exp_up": exp_up, "exp_down": exp_down, "dense_gate": dense_gate, "dense_up": dense_up, "dense_down": dense_down, "branch_gate": branch_gate}


EPS = 1e-06

def rms_scale(values, scales):
    widened = values.astype(jnp.float32)
    scaled = widened * lax.rsqrt(lax.optimization_barrier(jnp.mean(widened * widened, axis=-1, keepdims=True)) + EPS)
    return (scaled * scales.astype(jnp.float32)).astype(jnp.bfloat16)

def rotary_angles(positions, head_dim):
    halfway = head_dim // 2
    frequency = 10000.0 ** (-jnp.arange(halfway, dtype=jnp.float32) * 2.0 / head_dim)
    return positions.astype(jnp.float32)[:, None] * frequency[None, :]

def rotate_heads(values, angles):
    halfway = values.shape[-1] // 2
    cosine = jnp.cos(angles)[:, None, :]
    sine_of = jnp.sin(angles)[:, None, :]
    leading = values[..., :halfway]
    trailing = values[..., halfway:]
    return jnp.concatenate([leading * cosine - trailing * sine_of, trailing * cosine + leading * sine_of], axis=-1)

def log_decay(head_count):
    spread = jnp.arange(head_count, dtype=jnp.float32) * (5.0 / max(head_count - 1, 1))
    return jnp.log1p(-2.0 ** (-5.0 - spread))

def retain(queries, keys_in, values_in, gate_pre, old_state, positions, scales, log_gamma):
    row_count, head_count, head_dim = (old_state.shape[0], old_state.shape[1], old_state.shape[2])
    angles = rotary_angles(positions, head_dim)
    rot_query = rotate_heads(queries.astype(jnp.float32).reshape(row_count, head_count, head_dim), angles)
    rot_key = rotate_heads(keys_in.astype(jnp.float32).reshape(row_count, head_count, head_dim), angles) * head_dim ** (-0.5)
    value_heads = values_in.astype(jnp.float32).reshape(row_count, head_count, head_dim)
    new_state = jnp.exp(log_gamma)[None, :, None, None] * old_state + rot_key[:, :, :, None] * value_heads[:, :, None, :]
    readout = jnp.einsum('shd,shdv->shv', rot_query, new_state, precision=lax.Precision.HIGHEST)
    centred = readout - lax.optimization_barrier(jnp.mean(readout, axis=-1, keepdims=True))
    normed = centred * lax.rsqrt(lax.optimization_barrier(jnp.mean(centred * centred, axis=-1, keepdims=True)) + EPS)
    normed = normed * scales.astype(jnp.float32).reshape(head_count, head_dim)
    gated_out = normed.reshape(row_count, head_count * head_dim) * jax.nn.silu(gate_pre.astype(jnp.float32))
    return (gated_out.astype(jnp.bfloat16), new_state)

def expert_total(normed_ffn, route_ids, route_share, exp_gate, exp_up, exp_down):
    token_count = normed_ffn.shape[0]
    flat_ids = route_ids.reshape(-1)
    flat_share = route_share.reshape(-1)
    most_rows = N_EP * CAP

    def one_expert(running, expert):
        matches = flat_ids == expert
        where_hit = jnp.nonzero(matches, size=most_rows, fill_value=0)[0].astype(jnp.int32)
        in_use = jnp.arange(most_rows, dtype=jnp.int32) < jnp.sum(matches.astype(jnp.int32))
        token_of = (where_hit // TOP_K).astype(jnp.int32)
        chosen = normed_ffn[token_of]
        gate_part = jnp.dot(chosen, exp_gate[expert], preferred_element_type=jnp.float32)
        up_part = jnp.dot(chosen, exp_up[expert], preferred_element_type=jnp.float32)
        hidden = (jax.nn.silu(gate_part) * up_part).astype(jnp.bfloat16)
        result = jnp.dot(hidden, exp_down[expert], preferred_element_type=jnp.float32)
        picked = flat_share[where_hit]
        weight = jnp.where(in_use, picked, jnp.zeros_like(picked))
        return (running.at[token_of].add(result * weight[:, None]), None)
    running, _ = lax.scan(one_expert, jnp.zeros((token_count, D), jnp.float32), jnp.arange(EXPERTS, dtype=jnp.int32))
    return running

def reference(inputs, positions, ret_state, norm_mix, w_query, w_key, w_value, w_gate_in, head_gain, w_out, norm_ffn, route_ids, route_weight, exp_gate, exp_up, exp_down, dense_gate, dense_up, dense_down, branch_gate):
    normed = rms_scale(inputs, norm_mix)
    queries = jnp.dot(normed, w_query, preferred_element_type=jnp.float32).astype(jnp.bfloat16)
    keys_new = jnp.dot(normed, w_key, preferred_element_type=jnp.float32).astype(jnp.bfloat16)
    values_new = jnp.dot(normed, w_value, preferred_element_type=jnp.float32).astype(jnp.bfloat16)
    gate_pre = jnp.dot(normed, w_gate_in, preferred_element_type=jnp.float32).astype(jnp.bfloat16)
    retained, new_state = retain(queries, keys_new, values_new, gate_pre, ret_state, positions, head_gain, log_decay(HEADS))
    group_width = RET_WIDTH // N_TP
    halves = [lax.optimization_barrier(jnp.dot(retained[:, member * group_width:(member + 1) * group_width], w_out[member * group_width:(member + 1) * group_width], preferred_element_type=jnp.float32).astype(jnp.bfloat16)).astype(jnp.float32) for member in range(N_TP)]
    mixer_out = reduce(jnp.add, halves).astype(jnp.bfloat16)
    residual_sum = (inputs.astype(jnp.float32) + mixer_out.astype(jnp.float32)).astype(jnp.bfloat16)
    normed_ffn = rms_scale(residual_sum, norm_ffn)
    dense_hidden = (jax.nn.silu(jnp.dot(normed_ffn, dense_gate, preferred_element_type=jnp.float32)) * jnp.dot(normed_ffn, dense_up, preferred_element_type=jnp.float32)).astype(jnp.bfloat16)
    dense_result = jnp.dot(dense_hidden, dense_down, preferred_element_type=jnp.float32)
    branch_open = jax.nn.sigmoid(jnp.dot(normed_ffn, branch_gate[:, None], preferred_element_type=jnp.float32))
    widened = route_weight.astype(jnp.float32)
    route_share = widened / lax.optimization_barrier(jnp.sum(widened, axis=-1, keepdims=True))
    experts_out = expert_total(normed_ffn, route_ids, route_share, exp_gate, exp_up, exp_down)
    layer_out = (residual_sum.astype(jnp.float32) + experts_out + branch_open * dense_result).astype(jnp.bfloat16)
    return (layer_out, new_state)
```

```python
import jax
import jax.numpy as jnp
from jax import lax
from jax.experimental import pallas as pl
from jax.experimental.pallas import tpu as pltpu
from jax.sharding import Mesh, PartitionSpec as P

D = 2048
HEADS = 12
EPS = 1e-06
F32 = jnp.float32
BF16 = jnp.bfloat16

RIGHT = [(i, (i + 1) % 4) for i in range(4)]
LEFT = [(i, (i - 1) % 4) for i in range(4)]
ACROSS = [(i, (i + 2) % 4) for i in range(4)]
SWAP = [(0, 1), (1, 0)]


def rms_scale(values, scales):
    widened = values.astype(F32)
    scaled = widened * lax.rsqrt(jnp.mean(widened * widened, axis=-1, keepdims=True) + EPS)
    return (scaled * scales.astype(F32)).astype(BF16)


def ring_gather(own, cut):
    from_left = lax.ppermute(own, "x", RIGHT)
    from_right = lax.ppermute(own, "x", LEFT)
    far_a = lax.ppermute(from_left[:cut], "x", RIGHT)
    far_b = lax.ppermute(from_right[cut:], "x", LEFT)
    return own, from_left, from_right, far_a, far_b


def project_body(xi_ref, x_ref, own, left, right, far_a, far_b, out_ref, wide):
    p = pl.program_id(0)
    xi = xi_ref[0]

    def place(offset, value):
        at = pl.multiple_of(((xi + offset) % 4) * 32, 32)
        wide[pl.ds(at, 32), :] = value

    place(0, own[0])
    place(3, left[0])
    place(1, right[0])

    @pl.when(p < 2)
    def _():
        place(2, far_a[0])

    @pl.when(p >= 2)
    def _():
        place(2, far_b[0])

    out_ref[...] = jnp.dot(x_ref[...], wide[...], preferred_element_type=F32).astype(BF16)


def project(xi, tokens, chunks):
    rows, inner = tokens.shape
    width = chunks[0].shape[2]
    one = lambda index: pl.BlockSpec((1, 32, width), index)
    return pl.pallas_call(
        project_body,
        grid=(4,),
        in_specs=[
            pl.BlockSpec(memory_space=pltpu.SMEM),
            pl.BlockSpec((rows, inner), lambda p: (0, 0)),
            one(lambda p: (p, 0, 0)),
            one(lambda p: (p, 0, 0)),
            one(lambda p: (p, 0, 0)),
            one(lambda p: (jnp.minimum(p, 1), 0, 0)),
            one(lambda p: (jnp.maximum(p - 2, 0), 0, 0)),
        ],
        out_specs=pl.BlockSpec((rows, width), lambda p: (0, p)),
        out_shape=jax.ShapeDtypeStruct((rows, 4 * width), BF16),
        scratch_shapes=[pltpu.VMEM((inner, width), BF16)],
        name="project",
    )(xi, tokens, *chunks)


PER_STEP = 2


def retain_body(
    xi_ref, gamma_ref, parts, cosine, sine, gain, state, own, left, right, far_a, far_b,
    new_state, mixed, queries_keys, values, gates, readouts, retained, w_full, sems,
):
    step = pl.program_id(0)
    xi = xi_ref[0]

    def copies():
        out = []
        for offset, ref, lo, n in ((0, own, 0, 16), (3, left, 0, 16), (1, right, 0, 16), (2, far_a, 0, 8), (2, far_b, 8, 8)):
            for h in range(6):
                out.append(
                    pltpu.make_async_copy(
                        ref.at[:, h],
                        w_full.at[pl.ds(lo, n), (xi + offset) % 4, :, pl.ds(h * 128, 128)],
                        sems.at[len(out)],
                    )
                )
        return out

    @pl.when(step == 0)
    def _():
        for c in copies():
            c.start()
        cos_v, sin_v = cosine[...], sine[...]
        for h in range(6):
            def total(which):
                at = which * 768 + h * 128
                acc = parts[0, :, at : at + 128].astype(F32)
                for s in range(1, 16):
                    acc = acc + parts[s, :, at : at + 128].astype(F32)
                return acc.astype(BF16).astype(F32)

            q, k, v, g = (total(i) for i in range(4))
            queries_keys[:, h, :] = q * cos_v + pltpu.roll(q, 64, 1) * sin_v
            queries_keys[:, 8 + h, :] = (k * cos_v + pltpu.roll(k, 64, 1) * sin_v) * (128.0 ** -0.5)
            values[:, h, :] = v
            gates[:, h * 128 : (h + 1) * 128] = g * jax.nn.sigmoid(g)

    for i in range(PER_STEP):
        t = step * PER_STEP + i
        cols = jnp.transpose(queries_keys[t])
        for h in range(6):
            q_col = cols[:, h : h + 1]
            k_col = cols[:, 8 + h : 9 + h]
            v_row = values[t, h : h + 1, :]
            fresh = gamma_ref[h] * state[i, h] + k_col * v_row
            new_state[i, h] = fresh
            readouts[t, h : h + 1, :] = jnp.sum(q_col * fresh, axis=0, keepdims=True)

    @pl.when(step == pl.num_programs(0) - 1)
    def _():
        for h in range(6):
            at = slice(h * 128, (h + 1) * 128)
            r = readouts[:, h, :]
            centred = r - jnp.mean(r, axis=-1, keepdims=True)
            unit = centred * lax.rsqrt(jnp.mean(centred * centred, axis=-1, keepdims=True) + EPS)
            retained[:, at] = (unit * gain[:, at].astype(F32) * gates[:, at]).astype(BF16)
        for c in copies():
            c.wait()
        w = w_full[...].reshape(2048, 768)
        mixed[...] = lax.dot_general(
            retained[...], w, (((1,), (1,)), ((), ())), preferred_element_type=F32
        ).astype(BF16)


def retain(xi, gamma, parts, cosine, sine, gain, state, chunks):
    whole = lambda shape: pl.BlockSpec(shape, lambda s: (0,) * len(shape))
    anywhere = pl.BlockSpec(memory_space=pl.ANY)
    smem = pl.BlockSpec(memory_space=pltpu.SMEM)
    block = pl.BlockSpec((PER_STEP, 6, 128, 128), lambda s: (s, 0, 0, 0))
    return pl.pallas_call(
        retain_body,
        grid=(16 // PER_STEP,),
        in_specs=[
            smem, smem, whole((16, 16, 3072)), whole((16, 128)), whole((16, 128)), whole((1, 768)), block,
        ] + [anywhere] * 5,
        out_specs=[block, whole((16, 2048))],
        out_shape=[
            jax.ShapeDtypeStruct((16, 6, 128, 128), F32),
            jax.ShapeDtypeStruct((16, 2048), BF16),
        ],
        scratch_shapes=[
            pltpu.VMEM((16, 16, 128), F32),
            pltpu.VMEM((16, 8, 128), F32),
            pltpu.VMEM((16, 768), F32),
            pltpu.VMEM((16, 8, 128), F32),
            pltpu.VMEM((16, 768), BF16),
            pltpu.VMEM((16, 4, 32, 768), BF16),
            pltpu.SemaphoreType.DMA((30,)),
        ],
        name="retain",
    )(xi, gamma, parts, cosine, sine, gain, state, *chunks)


def to_all(array, axis):
    size = lax.axis_size(axis)
    copies = jnp.broadcast_to(array, (size, *array.shape))
    return lax.all_to_all(copies, axis, split_axis=0, concat_axis=0, tiled=True)


PLANE = ("z", "y")


def on_device(
    inputs, positions, ret_state, norm_mix, w_query, w_key, w_value, w_gate_in, head_gain, w_out,
    norm_ffn, route_ids, route_weight, exp_gate, exp_up, exp_down, dense_gate, dense_up, dense_down,
    branch_gate,
):
    x_at = lax.axis_index("x")
    zy_at = lax.axis_index(PLANE)
    xi = x_at.astype(jnp.int32).reshape(1)

    w4 = jnp.stack([w_query, w_key, w_value, w_gate_in])
    chunks = ring_gather(w4, 2)

    normed = rms_scale(inputs, norm_mix)
    pieces = normed.reshape(16, 16, 128).transpose(1, 0, 2)
    w_cols = w_out.T.reshape(32, 6, 128).transpose(1, 0, 2).reshape(192, 128)
    routes = jnp.concatenate([route_ids.astype(BF16), route_weight], axis=1)
    routes = jnp.pad(routes, ((0, 0), (0, 120)))
    shared = jnp.concatenate([w_cols, routes], axis=0)
    sent = jnp.concatenate([pieces, jnp.broadcast_to(shared, (16, 208, 128))], axis=1)
    got = lax.all_to_all(sent, PLANE, split_axis=0, concat_axis=0, tiled=True)
    tokens = got[:, :16].reshape(256, 128)
    w_plane = got[:, 16:208].reshape(16, 6, 32, 128)
    routed = got[:, 208:, :8].reshape(256, 8).astype(F32)

    partial = project(xi, tokens, chunks).reshape(16, 16, 3072)
    parts = lax.all_to_all(partial, PLANE, split_axis=0, concat_axis=0, tiled=True)

    out_chunks = ring_gather(w_plane, 8)
    dense = jnp.stack([dense_gate.T, dense_up.T, dense_down])
    dense, _ = lax.optimization_barrier((dense, chunks[3]))
    dense_chunks = ring_gather(dense.reshape(96, 2048), 48)

    ids = routed[:, :4]
    weights = routed[:, 4:]
    share = weights / jnp.sum(weights, axis=-1, keepdims=True)
    wanted = (zy_at * 4 + (x_at + jnp.arange(4)) % 4).astype(F32)
    hits = (ids[:, :, None] == wanted[None, None, :]).astype(F32)
    match = jnp.sum(hits, axis=1)
    share_of = jnp.sum(hits * share[:, :, None], axis=1)
    t = jnp.arange(256)
    before = ((t[:, None] // 16 == t[None, :] // 16) & (t[None, :] < t[:, None])).astype(BF16)
    rank = jnp.dot(before, match.astype(BF16), preferred_element_type=F32)
    slot = jnp.arange(32)
    place = (
        (t[:, None, None] // 16 == slot[None, None, :] // 2)
        & (rank[:, :, None] == (slot % 2).astype(F32)[None, None, :])
        & (match[:, :, None] > 0)
    )
    pick = place.astype(BF16).reshape(256, 128)
    weigh = jnp.where(place, share_of[:, :, None], 0.0).reshape(256, 128)
    weigh_hi = weigh.astype(BF16)
    weigh_lo = (weigh - weigh_hi.astype(F32)).astype(BF16)

    frequency = 10000.0 ** (-jnp.arange(64, dtype=F32) * 2.0 / 128)
    angles = positions.astype(F32)[:, None] * frequency[None, :]
    cos_v, sin_v = jnp.cos(angles), jnp.sin(angles)
    cosine = jnp.concatenate([cos_v, cos_v], axis=1)
    sine = jnp.concatenate([-sin_v, sin_v], axis=1)
    spread = jnp.arange(HEADS, dtype=F32) * (5.0 / (HEADS - 1))
    gamma = lax.dynamic_slice_in_dim(
        jnp.exp(jnp.log1p(-(2.0 ** (-5.0 - spread)))), lax.axis_index("tp") * 6, 6
    )
    new_state, mixed = retain(
        xi, gamma, parts, cosine, sine, head_gain.reshape(1, 768), ret_state, out_chunks
    )
    other = lax.ppermute(mixed, "tp", SWAP)
    mixer_out = (mixed.astype(F32) + other.astype(F32)).astype(BF16)
    residual_sum = (inputs.astype(F32) + mixer_out.astype(F32)).astype(BF16)
    normed_ffn = rms_scale(residual_sum, norm_ffn)

    plane = to_all(normed_ffn, PLANE).reshape(256, D)
    chosen = lax.dot_general(
        pick, plane, (((0,), (0,)), ((), ())), preferred_element_type=F32
    ).astype(BF16).reshape(4, 32, D)
    arrived = jnp.concatenate(
        [
            chosen[0],
            lax.ppermute(chosen[1], "x", RIGHT),
            lax.ppermute(chosen[2], "x", ACROSS),
            lax.ppermute(chosen[3], "x", LEFT),
        ],
        axis=0,
    )

    own, left, right, far_a, far_b = dense_chunks
    far = jnp.concatenate([far_a, far_b], axis=0)
    d_all = jnp.stack([own, left, right, far]).reshape(4, 3, 32, D)
    d_gate = d_all[:, 0].reshape(128, D)
    d_up = d_all[:, 1].reshape(128, D)
    d_down = d_all[:, 2].reshape(128, D)
    nt = (((1,), (1,)), ((), ()))
    gate_part = lax.dot_general(plane, d_gate, nt, preferred_element_type=F32)
    up_part = lax.dot_general(plane, d_up, nt, preferred_element_type=F32)
    dense_hidden = (jax.nn.silu(gate_part) * up_part).astype(BF16)
    opening = jax.nn.sigmoid(
        jnp.sum(plane.astype(F32) * branch_gate.astype(F32)[None, :], axis=-1, keepdims=True)
    )

    gate_part = jnp.dot(arrived, exp_gate[0], preferred_element_type=F32)
    up_part = jnp.dot(arrived, exp_up[0], preferred_element_type=F32)
    hidden = (jax.nn.silu(gate_part) * up_part).astype(BF16)
    result = jnp.dot(hidden, exp_down[0], preferred_element_type=F32).astype(BF16).reshape(4, 32, D)
    returned = jnp.concatenate(
        [
            result[0],
            lax.ppermute(result[1], "x", LEFT),
            lax.ppermute(result[2], "x", ACROSS),
            lax.ppermute(result[3], "x", RIGHT),
        ],
        axis=0,
    )
    dense_part = jnp.dot(dense_hidden, d_down, preferred_element_type=F32) * opening
    branch = (
        dense_part
        + jnp.dot(weigh_hi, returned, preferred_element_type=F32)
        + jnp.dot(weigh_lo, returned, preferred_element_type=F32)
    ).astype(BF16).reshape(16, 16, D)
    summed = jnp.sum(
        lax.all_to_all(branch, PLANE, split_axis=0, concat_axis=0, tiled=True).astype(F32), axis=0
    ).astype(BF16)
    total = summed.astype(F32) + lax.ppermute(summed, "tp", SWAP).astype(F32)
    layer_out = (residual_sum.astype(F32) + total).astype(BF16)
    return (layer_out, new_state)


EP = ("z", "y", "x")


def solution(mesh):
    inner = Mesh(mesh.devices.reshape(4, 4, 4, 2), ("z", "y", "x", "tp"))
    in_specs = (
        P(EP, None),
        P(EP),
        P(EP, "tp", None, None),
        P(),
        P(EP, "tp"),
        P(EP, "tp"),
        P(EP, "tp"),
        P(EP, "tp"),
        P("tp"),
        P("tp", EP),
        P(),
        P(EP, None),
        P(EP, None),
        P(EP, None, "tp"),
        P(EP, None, "tp"),
        P(EP, "tp", None),
        P(None, (*EP, "tp")),
        P(None, (*EP, "tp")),
        P((*EP, "tp"), None),
        P(),
    )
    out_specs = (P(EP, None), P(EP, "tp", None, None))
    return jax.shard_map(
        on_device, mesh=inner, in_specs=in_specs, out_specs=out_specs, check_vma=False
    )
```

```python
import jax
import jax.numpy as jnp
from jax import lax
from jax.experimental import pallas as pl
from jax.experimental.pallas import tpu as pltpu
from jax.sharding import Mesh, PartitionSpec as P


D = 2048
HEADS = 12
EPS = 1e-06
F32 = jnp.float32
BF16 = jnp.bfloat16

RIGHT = [(i, (i + 1) % 4) for i in range(4)]
LEFT = [(i, (i - 1) % 4) for i in range(4)]
ACROSS = [(i, (i + 2) % 4) for i in range(4)]
SWAP = [(0, 1), (1, 0)]
PLANE = ("z", "y")
NT = (((1,), (1,)), ((), ()))


def ring_gather(own):
    return (
        own,
        lax.ppermute(own, "x", RIGHT),
        lax.ppermute(own, "x", ACROSS),
        lax.ppermute(own, "x", LEFT),
    )


OFFSETS = (0, 3, 2, 1)


def whole(shape):
    return pl.BlockSpec(shape, lambda *s: (0,) * len(shape))


SMEM = pl.BlockSpec(memory_space=pltpu.SMEM)


def prepare_body(x_ref, gain, ids, shares, wq, wk, wv, wg, sent, w4, routes):
    w4[0] = wq[...]
    w4[1] = wk[...]
    w4[2] = wv[...]
    w4[3] = wg[...]
    routes[...] = jnp.zeros((16, 128), F32)
    routes[:, 0:4] = ids[...].astype(F32)
    routes[:, 4:8] = shares[...].astype(F32)
    route = routes[...].astype(BF16)
    x = x_ref[...]
    v = x.astype(F32)
    scaled = v * lax.rsqrt(jnp.mean(v * v, axis=-1, keepdims=True) + EPS)
    normed = (scaled * gain[...].astype(F32).reshape(1, D)).astype(BF16)
    for j in range(16):
        at = slice(j * 128, (j + 1) * 128)
        sent[j, 0:16, :] = normed[:, at]
        sent[j, 16:32, :] = x[:, at]
        sent[j, 32:48, :] = route


def prepare(x, gain, ids, shares, ws):
    return pl.pallas_call(
        prepare_body,
        out_shape=[
            jax.ShapeDtypeStruct((16, 48, 128), BF16),
            jax.ShapeDtypeStruct((4, 32, 768), BF16),
        ],
        scratch_shapes=[pltpu.VMEM((16, 128), F32)],
        name="prepare",
    )(x, gain, ids, shares, *ws)


def project_body(xi_ref, x_ref, c0, c1, c2, c3, out_ref, wide):
    xi = xi_ref[0]
    for offset, chunk in zip(OFFSETS, (c0, c1, c2, c3)):
        at = pl.multiple_of(((xi + offset) % 4) * 32, 32)
        wide[pl.ds(at, 32), :] = chunk[0]
    x = x_ref[:, 0:16, :].reshape(256, 128)
    out = jnp.dot(x, wide[...], preferred_element_type=F32).astype(BF16)
    out_ref[...] = out.reshape(16, 16, 768)


def project(xi, got, chunks):
    one = pl.BlockSpec((1, 32, 768), lambda p: (p, 0, 0))
    return pl.pallas_call(
        project_body,
        grid=(4,),
        in_specs=[SMEM, whole((16, 48, 128)), one, one, one, one],
        out_specs=pl.BlockSpec((16, 16, 768), lambda p: (0, 0, p)),
        out_shape=jax.ShapeDtypeStruct((16, 16, 3072), BF16),
        scratch_shapes=[pltpu.VMEM((128, 768), BF16)],
        name="project",
    )(xi, got, *chunks)


PER_STEP = 2
STEPS = 16 // PER_STEP


def retain_body(
    gamma_ref, parts_ref, cosine, sine, gain, state_ref,
    new_state, sent, parts, buf, queries_keys, values, gates, readouts, sems,
):
    fetch_parts = pltpu.make_async_copy(parts_ref, parts, sems.at[2 * STEPS])
    fetch_parts.start()

    def rows(i):
        return pl.ds(i * PER_STEP, PER_STEP)

    def fetch(i):
        return pltpu.make_async_copy(state_ref.at[rows(i)], buf.at[rows(i)], sems.at[i])

    def store(i):
        return pltpu.make_async_copy(buf.at[rows(i)], new_state.at[rows(i)], sems.at[STEPS + i])

    for i in range(STEPS):
        fetch(i).start()
    fetch_parts.wait()
    cos_v, sin_v = cosine[...], sine[...]
    for h in range(6):
        def total(which):
            at = which * 768 + h * 128
            acc = parts[0, :, at : at + 128].astype(F32)
            for s in range(1, 16):
                acc = acc + parts[s, :, at : at + 128].astype(F32)
            return acc.astype(BF16).astype(F32)

        q, k, v, g = (total(i) for i in range(4))
        queries_keys[:, h, :] = q * cos_v + pltpu.roll(q, 64, 1) * sin_v
        queries_keys[:, 8 + h, :] = (k * cos_v + pltpu.roll(k, 64, 1) * sin_v) * (128.0 ** -0.5)
        values[:, h, :] = v
        gates[:, h * 128 : (h + 1) * 128] = g * jax.nn.sigmoid(g)

    def some(i, carry):
        fetch(i).wait()
        for j in range(PER_STEP):
            t = i * PER_STEP + j
            cols = jnp.transpose(queries_keys[t])
            for h in range(6):
                q_col = cols[:, h : h + 1]
                k_col = cols[:, 8 + h : 9 + h]
                v_row = values[t, h : h + 1, :]
                fresh = gamma_ref[h] * buf[t, h] + k_col * v_row
                buf[t, h] = fresh
                readouts[t, h : h + 1, :] = jnp.sum(q_col * fresh, axis=0, keepdims=True)
        store(i).start()
        return carry

    lax.fori_loop(0, STEPS, some, 0)
    for h in range(6):
        at = slice(h * 128, (h + 1) * 128)
        r = readouts[:, h, :]
        centred = r - jnp.mean(r, axis=-1, keepdims=True)
        unit = centred * lax.rsqrt(jnp.mean(centred * centred, axis=-1, keepdims=True) + EPS)
        kept = (unit * gain[:, at].astype(F32) * gates[:, at]).astype(BF16)
        for s in range(16):
            sent[s, :, at] = kept
    for i in range(STEPS):
        store(i).wait()


def retain(gamma, parts, cosine, sine, gain, state):
    anywhere = pl.BlockSpec(memory_space=pl.ANY)
    vmem = pl.BlockSpec(memory_space=pltpu.VMEM)
    return pl.pallas_call(
        retain_body,
        in_specs=[SMEM, anywhere, vmem, vmem, vmem, anywhere],
        out_specs=[anywhere, vmem],
        out_shape=[
            jax.ShapeDtypeStruct((16, 6, 128, 128), F32),
            jax.ShapeDtypeStruct((16, 16, 768), BF16),
        ],
        scratch_shapes=[
            pltpu.VMEM((16, 16, 3072), BF16),
            pltpu.VMEM((16, 6, 128, 128), F32),
            pltpu.VMEM((16, 16, 128), F32),
            pltpu.VMEM((16, 8, 128), F32),
            pltpu.VMEM((16, 768), F32),
            pltpu.VMEM((16, 8, 128), F32),
            pltpu.SemaphoreType.DMA((2 * STEPS + 1,)),
        ],
        name="retain",
    )(gamma, parts, cosine, sine, gain, state)


def mix_body(xi_ref, kept, c0, c1, c2, c3, out_ref, wide):
    xi = xi_ref[0]
    for offset, chunk in zip(OFFSETS, (c0, c1, c2, c3)):
        at = pl.multiple_of(((xi + offset) % 4) * 32, 32)
        wide[pl.ds(at, 32), :] = chunk[...]
    rows = kept[...].reshape(256, 768)
    out_ref[...] = lax.dot_general(rows, wide[...], NT, preferred_element_type=F32).astype(BF16)


def mix(xi, kept, chunks):
    vmem = pl.BlockSpec(memory_space=pltpu.VMEM)
    return pl.pallas_call(
        mix_body,
        in_specs=[SMEM] + [vmem] * 5,
        out_shape=jax.ShapeDtypeStruct((256, 128), BF16),
        scratch_shapes=[pltpu.VMEM((128, 768), BF16)],
        name="mix",
    )(xi, kept, *chunks)


def spread_body(zy_ref, res, gain, branch, pick, plane, s0, s1, s2, s3, opening, own):
    total = jnp.zeros((256, 128), F32)
    for s in range(16):
        r = res[s].astype(F32)
        total = total + r * r
    scale = lax.rsqrt(jnp.sum(total, axis=-1, keepdims=True) / D + EPS)
    first = pl.multiple_of(zy_ref[0] * 16, 16)
    dots = jnp.zeros((256, 128), F32)
    for s in range(16):
        at = slice(s * 128, (s + 1) * 128)
        n = (res[s].astype(F32) * scale * gain[s : s + 1, :].astype(F32)).astype(BF16)
        plane[:, at] = n
        dots = dots + n.astype(F32) * branch[s : s + 1, :].astype(F32)
        rows = jnp.dot(pick[...], n, preferred_element_type=F32).astype(BF16)
        for k, out in enumerate((s0, s1, s2, s3)):
            out[:, at] = rows[k * 32 : (k + 1) * 32]
        own[:, at] = res[s, pl.ds(first, 16), :]
    opening[...] = jax.nn.sigmoid(jnp.sum(dots, axis=-1, keepdims=True))


def spread(zy, res, gain, branch, pick):
    vmem = pl.BlockSpec(memory_space=pltpu.VMEM)
    rows = jax.ShapeDtypeStruct((32, D), BF16)
    return pl.pallas_call(
        spread_body,
        in_specs=[SMEM] + [vmem] * 4,
        out_shape=[
            jax.ShapeDtypeStruct((256, D), BF16), rows, rows, rows, rows,
            jax.ShapeDtypeStruct((256, 1), F32),
            jax.ShapeDtypeStruct((16, D), BF16),
        ],
        name="spread",
    )(zy, res, gain, branch, pick)


def dense_body(plane, c0, c1, c2, c3, hidden, gate, up):
    for r, chunk in enumerate((c0, c1, c2, c3)):
        at = slice(r * 32, (r + 1) * 32)
        gate[at, :] = chunk[0:32, :]
        up[at, :] = chunk[32:64, :]
    x = plane[...]
    g = lax.dot_general(x, gate[...], NT, preferred_element_type=F32)
    u = lax.dot_general(x, up[...], NT, preferred_element_type=F32)
    hidden[...] = (g * jax.nn.sigmoid(g) * u).astype(BF16)


def dense_first(plane, chunks):
    return pl.pallas_call(
        dense_body,
        out_shape=jax.ShapeDtypeStruct((256, 128), BF16),
        scratch_shapes=[pltpu.VMEM((128, D), BF16), pltpu.VMEM((128, D), BF16)],
        name="dense_first",
    )(plane, *chunks)


CUT = 4


def expert_body(
    a0, a1, a2, a3, gate_ref, up_ref, down_ref, r0, r1, r2, r3, rows, gate, up, down, sems
):
    def fetch(ref, to, i, sem):
        n = to.shape[0] // CUT
        at = pl.ds(i * n, n)
        return pltpu.make_async_copy(ref.at[0, at], to.at[at], sems.at[sem])

    first = [(fetch(gate_ref, gate, i, i), fetch(up_ref, up, i, CUT + i)) for i in range(CUT)]
    second = [fetch(down_ref, down, i, 2 * CUT + i) for i in range(CUT)]
    for g, u in first:
        g.start()
        u.start()
    for d in second:
        d.start()
    for k, a in enumerate((a0, a1, a2, a3)):
        rows[k * 32 : (k + 1) * 32, :] = a[...]
    g_sum = u_sum = None
    n = D // CUT
    for i, (g, u) in enumerate(first):
        at = slice(i * n, (i + 1) * n)
        g.wait()
        g_part = jnp.dot(rows[:, at], gate[at, :], preferred_element_type=F32)
        u.wait()
        u_part = jnp.dot(rows[:, at], up[at, :], preferred_element_type=F32)
        g_sum = g_part if g_sum is None else g_sum + g_part
        u_sum = u_part if u_sum is None else u_sum + u_part
    h = (g_sum * jax.nn.sigmoid(g_sum) * u_sum).astype(BF16)
    for d in second:
        d.wait()
    for j in range(4):
        at = slice(j * 512, (j + 1) * 512)
        out = jnp.dot(h, down[:, at], preferred_element_type=F32).astype(BF16)
        for k, r in enumerate((r0, r1, r2, r3)):
            r[:, at] = out[k * 32 : (k + 1) * 32, :]


def experts(arrived, gate, up, down):
    rows = jax.ShapeDtypeStruct((32, D), BF16)
    anywhere = pl.BlockSpec(memory_space=pl.ANY)
    vmem = pl.BlockSpec(memory_space=pltpu.VMEM)
    return pl.pallas_call(
        expert_body,
        in_specs=[vmem] * 4 + [anywhere] * 3,
        out_shape=[rows] * 4,
        scratch_shapes=[
            pltpu.VMEM((128, D), BF16),
            pltpu.VMEM((D, 512), BF16),
            pltpu.VMEM((D, 512), BF16),
            pltpu.VMEM((512, D), BF16),
            pltpu.SemaphoreType.DMA((3 * CUT,)),
        ],
        name="experts",
    )(*arrived, gate, up, down)


def combine_body(hidden, c0, c1, c2, c3, opening, weigh, b0, b1, b2, b3, out, down, back):
    for r, chunk in enumerate((c0, c1, c2, c3)):
        down[r * 32 : (r + 1) * 32, :] = chunk[64:96, :]
    for k, b in enumerate((b0, b1, b2, b3)):
        back[k * 32 : (k + 1) * 32, :] = b[...]
        back[128 + k * 32 : 128 + (k + 1) * 32, :] = b[...]
    opened = opening[...]
    for j in range(4):
        at = slice(j * 512, (j + 1) * 512)
        term = jnp.dot(hidden[...], down[:, at], preferred_element_type=F32) * opened
        term = term + jnp.dot(weigh[...], back[:, at], preferred_element_type=F32)
        out[:, :, at] = term.astype(BF16).reshape(16, 16, 512)


def combine(hidden, chunks, opening, weigh, back):
    return pl.pallas_call(
        combine_body,
        out_shape=jax.ShapeDtypeStruct((16, 16, D), BF16),
        scratch_shapes=[pltpu.VMEM((128, D), BF16), pltpu.VMEM((256, D), BF16)],
        name="combine",
    )(hidden, *chunks, opening, weigh, *back)


def plane_exchange(array):
    return lax.all_to_all(array, PLANE, split_axis=0, concat_axis=0, tiled=True)


def routing(routed, x_at, zy_at):
    ids = routed[:, :4]
    weights = routed[:, 4:8]
    share = weights / jnp.sum(weights, axis=-1, keepdims=True)
    wanted = (zy_at * 4 + (x_at + jnp.arange(4)) % 4).astype(F32)
    hits = (ids[:, :, None] == wanted[None, None, :]).astype(F32)
    match = jnp.sum(hits, axis=1)
    share_of = jnp.sum(hits * share[:, :, None], axis=1)
    t = jnp.arange(256)
    before = ((t[:, None] // 16 == t[None, :] // 16) & (t[None, :] < t[:, None])).astype(BF16)
    rank = jnp.dot(before, match.astype(BF16), preferred_element_type=F32)
    slot = jnp.arange(32)
    place = (
        (t[:, None, None] // 16 == slot[None, None, :] // 2)
        & (rank[:, :, None] == (slot % 2).astype(F32)[None, None, :])
        & (match[:, :, None] > 0)
    )
    pick = place.astype(BF16).reshape(256, 128).T
    weigh = jnp.where(place, share_of[:, :, None], 0.0).reshape(256, 128)
    high = weigh.astype(BF16)
    low = (weigh - high.astype(F32)).astype(BF16)
    return pick, jnp.concatenate([high, low], axis=1)


def on_device(
    inputs, positions, ret_state, norm_mix, w_query, w_key, w_value, w_gate_in, head_gain, w_out,
    norm_ffn, route_ids, route_weight, exp_gate, exp_up, exp_down, dense_gate, dense_up, dense_down,
    branch_gate,
):
    x_at = lax.axis_index("x")
    zy_at = lax.axis_index(PLANE)
    xi = x_at.astype(jnp.int32).reshape(1)
    zy = zy_at.astype(jnp.int32).reshape(1)

    sent, w4 = prepare(
        inputs, norm_mix, route_ids, route_weight, (w_query, w_key, w_value, w_gate_in)
    )
    chunks = ring_gather(w4)
    got = plane_exchange(sent)
    in_cols = got[:, 16:32].reshape(256, 128)
    routed = got[:, 32:48, :8].reshape(256, 8).astype(F32)

    partial = project(xi, got, chunks)
    parts = plane_exchange(partial)

    out_chunks = ring_gather(w_out.T)
    dense = jnp.concatenate([dense_gate.T, dense_up.T, dense_down], axis=0)
    dense_chunks = ring_gather(dense)
    pick, weigh = routing(routed, x_at, zy_at)
    parts, out_chunks, dense_chunks, pick, weigh = lax.optimization_barrier(
        (parts, out_chunks, dense_chunks, pick, weigh)
    )

    frequency = 10000.0 ** (-jnp.arange(64, dtype=F32) * 2.0 / 128)
    angles = positions.astype(F32)[:, None] * frequency[None, :]
    cos_v, sin_v = jnp.cos(angles), jnp.sin(angles)
    cosine = jnp.concatenate([cos_v, cos_v], axis=1)
    sine = jnp.concatenate([-sin_v, sin_v], axis=1)
    spreading = jnp.arange(HEADS, dtype=F32) * (5.0 / (HEADS - 1))
    gamma = lax.dynamic_slice_in_dim(
        jnp.exp(jnp.log1p(-(2.0 ** (-5.0 - spreading)))), lax.axis_index("tp") * 6, 6
    )
    new_state, kept = retain(gamma, parts, cosine, sine, head_gain.reshape(1, 768), ret_state)
    kept = plane_exchange(kept)
    mixed = mix(xi, kept, out_chunks)
    other = lax.ppermute(mixed, "tp", SWAP)
    mixer_out = (mixed.astype(F32) + other.astype(F32)).astype(BF16)
    res_cols = (in_cols.astype(F32) + mixer_out.astype(F32)).astype(BF16)
    res = plane_exchange(jnp.broadcast_to(res_cols, (16, 256, 128)))

    plane, s0, s1, s2, s3, opening, own_res = spread(
        zy, res, norm_ffn.reshape(16, 128), branch_gate.reshape(16, 128), pick
    )
    arrived = (
        s0,
        lax.ppermute(s1, "x", RIGHT),
        lax.ppermute(s2, "x", ACROSS),
        lax.ppermute(s3, "x", LEFT),
    )
    hidden = dense_first(plane, dense_chunks)
    r0, r1, r2, r3 = experts(arrived, exp_gate, exp_up, exp_down)
    back = (
        r0,
        lax.ppermute(r1, "x", LEFT),
        lax.ppermute(r2, "x", ACROSS),
        lax.ppermute(r3, "x", RIGHT),
    )
    branch = combine(hidden, dense_chunks, opening, weigh, back)
    terms = plane_exchange(branch)
    summed = jnp.sum(terms.astype(F32), axis=0).astype(BF16)
    total = summed.astype(F32) + lax.ppermute(summed, "tp", SWAP).astype(F32)
    layer_out = (own_res.astype(F32) + total).astype(BF16)
    return (layer_out, new_state)


EP = ("z", "y", "x")


def solution(mesh):
    inner = Mesh(mesh.devices.reshape(4, 4, 4, 2), ("z", "y", "x", "tp"))
    in_specs = (
        P(EP, None),
        P(EP),
        P(EP, "tp", None, None),
        P(),
        P(EP, "tp"),
        P(EP, "tp"),
        P(EP, "tp"),
        P(EP, "tp"),
        P("tp"),
        P("tp", EP),
        P(),
        P(EP, None),
        P(EP, None),
        P(EP, None, "tp"),
        P(EP, None, "tp"),
        P(EP, "tp", None),
        P(None, (*EP, "tp")),
        P(None, (*EP, "tp")),
        P((*EP, "tp"), None),
        P(),
    )
    out_specs = (P(EP, None), P(EP, "tp", None, None))
    return jax.shard_map(
        on_device, mesh=inner, in_specs=in_specs, out_specs=out_specs, check_vma=False
    )
```

```python
import jax
import jax.numpy as jnp
import numpy as np
from jax import lax
from jax.experimental import pallas as pl
from jax.experimental.pallas import tpu as pltpu
from jax.sharding import Mesh, PartitionSpec as P


D = 2048
HEADS = 12
EPS = 1e-06
F32 = jnp.float32
BF16 = jnp.bfloat16

RIGHT = [(i, (i + 1) % 4) for i in range(4)]
LEFT = [(i, (i - 1) % 4) for i in range(4)]
ACROSS = [(i, (i + 2) % 4) for i in range(4)]
SWAP = [(0, 1), (1, 0)]
PLANE = ("z", "y")
NT = (((1,), (1,)), ((), ()))
TN = (((0,), (0,)), ((), ()))
HBM = pl.BlockSpec(memory_space=pltpu.HBM)
VMEM = pl.BlockSpec(memory_space=pltpu.VMEM)


def ring_gather(own):
    return (
        own,
        lax.ppermute(own, "x", RIGHT),
        lax.ppermute(own, "x", ACROSS),
        lax.ppermute(own, "x", LEFT),
    )


OFFSETS = (0, 3, 2, 1)


SMEM = pl.BlockSpec(memory_space=pltpu.SMEM)


def prepare_body(x_ref, gain, ids, shares, wq, wk, wv, wg, sent, w4, routes):
    w4[0] = wq[...]
    w4[1] = wk[...]
    w4[2] = wv[...]
    w4[3] = wg[...]
    half = x_ref[pl.ds(pl.multiple_of(lax.axis_index("tp") * 8, 8), 8), :]
    routes[...] = jnp.zeros((8, 128), F32)
    routes[0:4, 0:16] = ids[...].astype(F32)
    routes[4:8, 0:16] = shares[...].astype(F32)
    first = lax.axis_index(PLANE) * 8
    turned = pltpu.roll(routes[...], (first - lax.axis_index("tp") * 8 + 128) % 128, 1)
    lane = lax.broadcasted_iota(jnp.int32, (8, 128), 1)
    route = jnp.where(lane // 8 == first // 8, turned, 0.0).astype(BF16)
    x = x_ref[...]
    v = x.astype(F32)
    scaled = v * lax.rsqrt(jnp.mean(v * v, axis=-1, keepdims=True) + EPS)
    normed = (scaled * gain[...].astype(F32).reshape(1, D)).astype(BF16)
    for j in range(16):
        at = slice(j * 128, (j + 1) * 128)
        sent[j, 0:16, :] = normed[:, at]
        sent[j, 16:24, :] = half[:, at]
        sent[j, 24:32, :] = route


def prepare(x, gain, ids, shares, ws):
    return pl.pallas_call(
        prepare_body,
        out_shape=[
            jax.ShapeDtypeStruct((16, 32, 128), BF16),
            jax.ShapeDtypeStruct((4, 32, 768), BF16),
        ],
        scratch_shapes=[pltpu.VMEM((8, 128), F32)],
        name="prepare",
    )(x, gain, ids, shares, *ws)


def project_body(x_ref, c0, c1, c2, c3, out_ref, wide, out, sems):
    xi = lax.axis_index("x")
    x = x_ref[:, 0:16, :].reshape(256, 128)
    stores = []
    for p in range(4):
        for offset, chunk in zip(OFFSETS, (c0, c1, c2, c3)):
            at = pl.multiple_of(((xi + offset) % 4) * 32, 32)
            wide[p, pl.ds(at, 32), :] = chunk[p]
        at = pl.ds(p * 768, 768)
        out[:, :, at] = (
            jnp.dot(x, wide[p], preferred_element_type=F32).astype(BF16).reshape(16, 16, 768)
        )
        stores.append(pltpu.make_async_copy(out.at[:, :, at], out_ref.at[:, :, at], sems.at[p]))
        stores[-1].start()
    for store in stores:
        store.wait()


def project(got, chunks):
    return pl.pallas_call(
        project_body,
        in_specs=[VMEM] * 5,
        out_specs=HBM,
        out_shape=jax.ShapeDtypeStruct((16, 16, 3072), BF16),
        scratch_shapes=[
            pltpu.VMEM((4, 128, 768), BF16),
            pltpu.VMEM((16, 16, 3072), BF16),
            pltpu.SemaphoreType.DMA((4,)),
        ],
        name="project",
    )(got, *chunks)


PER_STEP = 2
STEPS = 16 // PER_STEP
FREQUENCY = np.tile(10000.0 ** (-np.arange(64) * 2.0 / 128), 2).astype(np.float32)
TURN = np.repeat([-1.0, 1.0], 64).astype(np.float32)
GAMMA = [float(np.exp(np.log1p(-(2.0 ** (-5.0 - 5.0 * h / (HEADS - 1)))))) for h in range(HEADS)]


def retain_body(
    parts, cosine_ref, sine_ref, gain, state_ref, new_state, sent,
    buf, turns, queries_keys, values, gates, readouts, sems,
):
    fetch_turns = [
        pltpu.make_async_copy(cosine_ref, turns.at[0], sems.at[2 * STEPS]),
        pltpu.make_async_copy(sine_ref, turns.at[1], sems.at[2 * STEPS + 1]),
    ]
    for c in fetch_turns:
        c.start()
    upper = lax.axis_index("tp") == 1
    gamma = [jnp.where(upper, GAMMA[h + 6], GAMMA[h]).astype(F32) for h in range(6)]

    def rows(i):
        return pl.ds(i * PER_STEP, PER_STEP)

    def fetch(i):
        return pltpu.make_async_copy(state_ref.at[rows(i)], buf.at[rows(i)], sems.at[i])

    def store(i):
        return pltpu.make_async_copy(buf.at[rows(i)], new_state.at[rows(i)], sems.at[STEPS + i])

    for i in range(STEPS):
        fetch(i).start()
    for c in fetch_turns:
        c.wait()
    cos_v, sin_v = turns[0], turns[1]
    for h in range(6):
        def total(which):
            at = which * 768 + h * 128
            acc = parts[0, :, at : at + 128].astype(F32)
            for s in range(1, 16):
                acc = acc + parts[s, :, at : at + 128].astype(F32)
            return acc.astype(BF16).astype(F32)

        q, k, v, g = (total(i) for i in range(4))
        queries_keys[:, h, :] = q * cos_v + pltpu.roll(q, 64, 1) * sin_v
        queries_keys[:, 8 + h, :] = (k * cos_v + pltpu.roll(k, 64, 1) * sin_v) * (128.0 ** -0.5)
        values[:, h, :] = v
        gates[:, h * 128 : (h + 1) * 128] = g * jax.nn.sigmoid(g)

    def some(i, carry):
        fetch(i).wait()
        for j in range(PER_STEP):
            t = i * PER_STEP + j
            cols = jnp.transpose(queries_keys[t])
            for h in range(6):
                q_col = cols[:, h : h + 1]
                k_col = cols[:, 8 + h : 9 + h]
                v_row = values[t, h : h + 1, :]
                fresh = gamma[h] * buf[t, h] + k_col * v_row
                buf[t, h] = fresh
                readouts[t, h : h + 1, :] = jnp.sum(q_col * fresh, axis=0, keepdims=True)
        store(i).start()
        return carry

    lax.fori_loop(0, STEPS, some, 0)
    gains = gain[...].astype(F32).reshape(1, 768)
    for h in range(6):
        at = slice(h * 128, (h + 1) * 128)
        r = readouts[:, h, :]
        centred = r - jnp.mean(r, axis=-1, keepdims=True)
        unit = centred * lax.rsqrt(jnp.mean(centred * centred, axis=-1, keepdims=True) + EPS)
        kept = (unit * gains[:, at] * gates[:, at]).astype(BF16)
        for s in range(16):
            sent[s, :, at] = kept
    for i in range(STEPS):
        store(i).wait()


def retain(parts, cosine, sine, gain, state):
    return pl.pallas_call(
        retain_body,
        in_specs=[VMEM, HBM, HBM, VMEM, HBM],
        out_specs=[HBM, VMEM],
        out_shape=[
            jax.ShapeDtypeStruct((16, 6, 128, 128), F32),
            jax.ShapeDtypeStruct((16, 16, 768), BF16),
        ],
        scratch_shapes=[
            pltpu.VMEM((16, 6, 128, 128), F32),
            pltpu.VMEM((2, 16, 128), F32),
            pltpu.VMEM((16, 16, 128), F32),
            pltpu.VMEM((16, 8, 128), F32),
            pltpu.VMEM((16, 768), F32),
            pltpu.VMEM((16, 8, 128), F32),
            pltpu.SemaphoreType.DMA((2 * STEPS + 2,)),
        ],
        name="retain",
    )(parts, cosine, sine, gain, state)


def mix_body(kept, c0, c1, c2, c3, keep, give, wide, mixed):
    xi = lax.axis_index("x")
    core = lax.axis_index("tp")
    for offset, chunk in zip(OFFSETS, (c0, c1, c2, c3)):
        at = pl.multiple_of(((xi + offset) % 4) * 32, 32)
        wide[pl.ds(at, 32), :] = chunk[...]
    rows = kept[...].reshape(256, 768)
    out = lax.dot_general(rows, wide[...], NT, preferred_element_type=F32)
    mixed[...] = out.reshape(16, 16, 128)
    keep[...] = mixed[:, pl.ds(pl.multiple_of(core * 8, 8), 8), :].astype(BF16)
    give[...] = mixed[:, pl.ds(pl.multiple_of((1 - core) * 8, 8), 8), :].astype(BF16)


def mix(kept, chunks):
    half = jax.ShapeDtypeStruct((16, 8, 128), BF16)
    return pl.pallas_call(
        mix_body,
        in_specs=[VMEM] * 5,
        out_shape=[half, half],
        scratch_shapes=[pltpu.VMEM((128, 768), BF16), pltpu.VMEM((16, 16, 128), F32)],
        name="mix",
    )(kept, *chunks)


def settle_body(mine, other, got, out_ref):
    mixer_out = (mine[...].astype(F32) + other[...].astype(F32)).astype(BF16)
    res = (got[:, 16:24, :].astype(F32) + mixer_out.astype(F32)).astype(BF16).reshape(128, 128)
    for s in range(16):
        out_ref[s] = res


def settle(mine, other, got):
    return pl.pallas_call(
        settle_body,
        out_shape=jax.ShapeDtypeStruct((16, 128, 128), BF16),
        name="settle",
    )(mine, other, got)


def spread_body(res, gain, branch, pick, plane, s0, s1, s2, s3, opening, own):
    total = jnp.zeros((128, 128), F32)
    for s in range(16):
        r = res[s].astype(F32)
        total = total + r * r
    scale = lax.rsqrt(jnp.sum(total, axis=-1, keepdims=True) / D + EPS)
    first = pl.multiple_of(lax.axis_index(PLANE) * 8, 8)
    gains = gain[...].astype(F32).reshape(1, D)
    branches = branch[...].astype(F32).reshape(1, D)
    dots = jnp.zeros((128, 128), F32)
    for s in range(16):
        at = slice(s * 128, (s + 1) * 128)
        n = (res[s].astype(F32) * scale * gains[:, at]).astype(BF16)
        plane[:, at] = n
        dots = dots + n.astype(F32) * branches[:, at]
        rows = jnp.dot(pick[...], n, preferred_element_type=F32).astype(BF16)
        for k, out in enumerate((s0, s1, s2, s3)):
            out[:, at] = rows[k * 32 : (k + 1) * 32]
        own[:, at] = res[s, pl.ds(first, 8), :]
    opening[...] = jax.nn.sigmoid(jnp.sum(dots, axis=-1, keepdims=True))


def spread(res, gain, branch, pick):
    rows = jax.ShapeDtypeStruct((32, D), BF16)
    return pl.pallas_call(
        spread_body,
        in_specs=[VMEM] * 4,
        out_shape=[
            jax.ShapeDtypeStruct((128, D), BF16), rows, rows, rows, rows,
            jax.ShapeDtypeStruct((128, 1), F32),
            jax.ShapeDtypeStruct((8, D), BF16),
        ],
        name="spread",
    )(res, gain, branch, pick)


def dense_body(plane, c0, c1, c2, c3, c4, c5, c6, c7, hidden, gate, up):
    for r, chunk in enumerate((c0, c1, c2, c3, c4, c5, c6, c7)):
        at = slice(r * 32, (r + 1) * 32)
        gate[at, :] = chunk[0:32, :]
        up[at, :] = chunk[32:64, :]
    x = plane[...]
    g = lax.dot_general(x, gate[...], NT, preferred_element_type=F32)
    u = lax.dot_general(x, up[...], NT, preferred_element_type=F32)
    hidden[...] = (g * jax.nn.sigmoid(g) * u).astype(BF16)


def dense_first(plane, chunks):
    return pl.pallas_call(
        dense_body,
        out_shape=jax.ShapeDtypeStruct((128, 256), BF16),
        scratch_shapes=[pltpu.VMEM((256, D), BF16), pltpu.VMEM((256, D), BF16)],
        name="dense_first",
    )(plane, *chunks)


CUT = 4


def expert_body(
    a0, a1, a2, a3, gate_a, gate_b, up_a, up_b, down_a, down_b, r0, r1, r2, r3,
    rows, gate, up, down, sems,
):
    halves = []
    for w, (g_ref, u_ref, d_ref) in enumerate(((gate_a, up_a, down_a), (gate_b, up_b, down_b))):
        base = w * 3 * CUT
        gu, dn = [], []
        for i in range(CUT):
            n, m = D // CUT, 512 // CUT
            at, low = pl.ds(i * n, n), pl.ds(i * m, m)
            gu.append((
                pltpu.make_async_copy(g_ref.at[0, at], gate.at[w, at], sems.at[base + i]),
                pltpu.make_async_copy(u_ref.at[0, at], up.at[w, at], sems.at[base + CUT + i]),
            ))
            dn.append(
                pltpu.make_async_copy(d_ref.at[0, low], down.at[w, low], sems.at[base + 2 * CUT + i])
            )
        halves.append((gu, dn))
    for gu, _ in halves:
        for g, u in gu:
            g.start()
            u.start()
    for _, dn in halves:
        for d in dn:
            d.start()
    for k, a in enumerate((a0, a1, a2, a3)):
        rows[k * 32 : (k + 1) * 32, :] = a[...]
    n = D // CUT
    hidden = []
    for w, (gu, _) in enumerate(halves):
        g_sum = u_sum = None
        for i, (g, u) in enumerate(gu):
            at = slice(i * n, (i + 1) * n)
            g.wait()
            g_part = jnp.dot(rows[:, at], gate[w, at, :], preferred_element_type=F32)
            u.wait()
            u_part = jnp.dot(rows[:, at], up[w, at, :], preferred_element_type=F32)
            g_sum = g_part if g_sum is None else g_sum + g_part
            u_sum = u_part if u_sum is None else u_sum + u_part
        hidden.append((g_sum * jax.nn.sigmoid(g_sum) * u_sum).astype(BF16))
    for _, dn in halves:
        for d in dn:
            d.wait()
    for j in range(4):
        at = slice(j * 512, (j + 1) * 512)
        out = jnp.dot(hidden[0], down[0, :, at], preferred_element_type=F32)
        out = (out + jnp.dot(hidden[1], down[1, :, at], preferred_element_type=F32)).astype(BF16)
        for k, r in enumerate((r0, r1, r2, r3)):
            r[:, at] = out[k * 32 : (k + 1) * 32, :]


def experts(arrived, weights):
    rows = jax.ShapeDtypeStruct((32, D), BF16)
    return pl.pallas_call(
        expert_body,
        in_specs=[VMEM] * 4 + [HBM] * 6,
        out_shape=[rows] * 4,
        scratch_shapes=[
            pltpu.VMEM((128, D), BF16),
            pltpu.VMEM((2, D, 512), BF16),
            pltpu.VMEM((2, D, 512), BF16),
            pltpu.VMEM((2, 512, D), BF16),
            pltpu.SemaphoreType.DMA((6 * CUT,)),
        ],
        name="experts",
    )(*arrived, *weights)


def combine_body(
    hidden, c0, c1, c2, c3, c4, c5, c6, c7, opening, weigh, b0, b1, b2, b3, out, down, back
):
    for r, chunk in enumerate((c0, c1, c2, c3, c4, c5, c6, c7)):
        down[r * 32 : (r + 1) * 32, :] = chunk[64:96, :]
    for k, b in enumerate((b0, b1, b2, b3)):
        back[k * 32 : (k + 1) * 32, :] = b[...]
        back[128 + k * 32 : 128 + (k + 1) * 32, :] = b[...]
    opened = opening[...]
    for j in range(4):
        at = slice(j * 512, (j + 1) * 512)
        term = jnp.dot(hidden[...], down[:, at], preferred_element_type=F32) * opened
        term = term + lax.dot_general(weigh[...], back[:, at], TN, preferred_element_type=F32)
        out[:, :, at] = term.astype(BF16).reshape(16, 8, 512)


def combine(hidden, chunks, opening, weigh, back):
    return pl.pallas_call(
        combine_body,
        out_shape=jax.ShapeDtypeStruct((16, 8, D), BF16),
        scratch_shapes=[pltpu.VMEM((256, D), BF16), pltpu.VMEM((256, D), BF16)],
        name="combine",
    )(hidden, *chunks, opening, weigh, *back)


def plane_exchange(array):
    return lax.all_to_all(array, PLANE, split_axis=0, concat_axis=0, tiled=True)


def routing_body(got, pick, weigh):
    total = got[0, 24:32, :].astype(F32)
    for s in range(1, 16):
        total = total + got[s, 24:32, :].astype(F32)
    ids, weights = total[0:4], total[4:8]
    share = weights / jnp.sum(weights, axis=0, keepdims=True)
    a = lax.broadcasted_iota(jnp.int32, (128, 128), 0)
    b = lax.broadcasted_iota(jnp.int32, (128, 128), 1)
    before = ((a // 8 == b // 8) & (a < b)).astype(F32).astype(BF16)
    slot = lax.broadcasted_iota(jnp.int32, (32, 128), 0)
    token = lax.broadcasted_iota(jnp.int32, (32, 128), 1)
    mine = slot // 2 == token // 8
    x_at = lax.axis_index("x")
    zy_at = lax.axis_index(PLANE)
    for k in range(4):
        wanted = (zy_at * 4 + (x_at + k) % 4).astype(F32)
        hits = (ids == wanted).astype(F32)
        match = jnp.sum(hits, axis=0, keepdims=True)
        share_of = jnp.sum(hits * share, axis=0, keepdims=True)
        many = jnp.broadcast_to(match, (32, 128))
        rank = jnp.dot(many.astype(BF16), before, preferred_element_type=F32)
        place = mine & (rank == (slot % 2).astype(F32)) & (many > 0)
        at = slice(k * 32, (k + 1) * 32)
        pick[at, :] = jnp.where(place, 1.0, 0.0).astype(BF16)
        value = jnp.where(place, jnp.broadcast_to(share_of, (32, 128)), 0.0)
        high = value.astype(BF16)
        weigh[at, :] = high
        weigh[k * 32 + 128 : k * 32 + 160, :] = (value - high.astype(F32)).astype(BF16)


def routing(got):
    return pl.pallas_call(
        routing_body,
        out_shape=[
            jax.ShapeDtypeStruct((128, 128), BF16),
            jax.ShapeDtypeStruct((256, 128), BF16),
        ],
        name="routing",
    )(got)


def on_device(
    inputs, positions, ret_state, norm_mix, w_query, w_key, w_value, w_gate_in, head_gain, w_out,
    norm_ffn, route_ids, route_weight, exp_gate, exp_up, exp_down, dense_gate, dense_up, dense_down,
    branch_gate,
):
    core = lax.axis_index("tp")

    sent, w4 = prepare(
        inputs, norm_mix, route_ids.T, route_weight.T, (w_query, w_key, w_value, w_gate_in)
    )
    chunks = ring_gather(w4)
    got = plane_exchange(sent)

    partial = project(got, chunks)
    partial, got, positions, w_out, dense_gate, dense_up, dense_down, expert_own = (
        lax.optimization_barrier(
            (
                partial, got, positions, w_out, dense_gate, dense_up, dense_down,
                (exp_gate, exp_up, exp_down),
            )
        )
    )
    parts = plane_exchange(partial)

    out_chunks = ring_gather(w_out.T)
    dense = jnp.concatenate([dense_gate.T, dense_up.T, dense_down], axis=0)
    dense_chunks = ring_gather(dense)
    expert_other = tuple(lax.ppermute(w, "tp", SWAP) for w in expert_own)
    dense_chunks = dense_chunks + tuple(lax.ppermute(c, "tp", SWAP) for c in dense_chunks)
    pick, weigh = routing(got)

    angles = positions.astype(F32)[:, None] * FREQUENCY[None, :]
    cosine = jnp.cos(angles)
    sine = jnp.sin(angles) * TURN[None, :]
    new_state, kept = retain(parts, cosine, sine, head_gain, ret_state)
    kept = plane_exchange(kept)
    kept, out_chunks, dense_chunks, expert_other, pick, weigh = lax.optimization_barrier(
        (kept, out_chunks, dense_chunks, expert_other, pick, weigh)
    )
    keep, give = mix(kept, out_chunks)
    settled = settle(keep, lax.ppermute(give, "tp", SWAP), got)
    res = plane_exchange(settled)

    plane, s0, s1, s2, s3, opening, own_res = spread(res, norm_ffn, branch_gate, pick)
    arrived = (
        s0,
        lax.ppermute(s1, "x", RIGHT),
        lax.ppermute(s2, "x", ACROSS),
        lax.ppermute(s3, "x", LEFT),
    )
    hidden = dense_first(plane, dense_chunks)
    weights = tuple(w for pair in zip(expert_own, expert_other) for w in pair)
    r0, r1, r2, r3 = experts(arrived, weights)
    back = (
        r0,
        lax.ppermute(r1, "x", LEFT),
        lax.ppermute(r2, "x", ACROSS),
        lax.ppermute(r3, "x", RIGHT),
    )
    branch = combine(hidden, dense_chunks, opening, weigh, back)
    terms = plane_exchange(branch)
    summed = jnp.sum(terms.astype(F32), axis=0)
    mine = (own_res.astype(F32) + summed).astype(BF16)
    other = lax.ppermute(mine, "tp", SWAP)
    layer_out = jnp.concatenate(
        [jnp.where(core == 0, mine, other), jnp.where(core == 0, other, mine)], axis=0
    )
    return (layer_out, new_state)


EP = ("z", "y", "x")


def solution(mesh):
    inner = Mesh(mesh.devices.reshape(4, 4, 4, 2), ("z", "y", "x", "tp"))
    in_specs = (
        P(EP, None),
        P(EP),
        P(EP, "tp", None, None),
        P(),
        P(EP, "tp"),
        P(EP, "tp"),
        P(EP, "tp"),
        P(EP, "tp"),
        P("tp"),
        P("tp", EP),
        P(),
        P(EP, None),
        P(EP, None),
        P(EP, None, "tp"),
        P(EP, None, "tp"),
        P(EP, "tp", None),
        P(None, (*EP, "tp")),
        P(None, (*EP, "tp")),
        P((*EP, "tp"), None),
        P(),
    )
    out_specs = (P(EP, None), P(EP, "tp", None, None))
    return jax.shard_map(
        on_device, mesh=inner, in_specs=in_specs, out_specs=out_specs, check_vma=False
    )
```

```python
import jax
import jax.numpy as jnp
import numpy as np
from jax import lax
from jax.experimental import pallas as pl
from jax.experimental.pallas import tpu as pltpu
from jax.sharding import Mesh, PartitionSpec as P


D = 2048
HEADS = 12
EPS = 1e-06
F32 = jnp.float32
BF16 = jnp.bfloat16

RIGHT = [(i, (i + 1) % 4) for i in range(4)]
LEFT = [(i, (i - 1) % 4) for i in range(4)]
ACROSS = [(i, (i + 2) % 4) for i in range(4)]
SWAP = [(0, 1), (1, 0)]
PLANE = ("z", "y")
NT = (((1,), (1,)), ((), ()))
TN = (((0,), (0,)), ((), ()))
HBM = pl.BlockSpec(memory_space=pltpu.HBM)
VMEM = pl.BlockSpec(memory_space=pltpu.VMEM)


def ring_gather(own):
    return (
        own,
        lax.ppermute(own, "x", RIGHT),
        lax.ppermute(own, "x", ACROSS),
        lax.ppermute(own, "x", LEFT),
    )


OFFSETS = (0, 3, 2, 1)


SMEM = pl.BlockSpec(memory_space=pltpu.SMEM)


def prepare_body(x_ref, gain, ids, shares, wq, wk, wv, wg, sent, w4, routes):
    w4[0] = wq[...]
    w4[1] = wk[...]
    w4[2] = wv[...]
    w4[3] = wg[...]
    half = x_ref[pl.ds(pl.multiple_of(lax.axis_index("tp") * 8, 8), 8), :]
    routes[...] = jnp.zeros((8, 128), F32)
    routes[0:4, 0:16] = ids[...].astype(F32)
    routes[4:8, 0:16] = shares[...].astype(F32)
    first = lax.axis_index(PLANE) * 8
    turned = pltpu.roll(routes[...], (first - lax.axis_index("tp") * 8 + 128) % 128, 1)
    lane = lax.broadcasted_iota(jnp.int32, (8, 128), 1)
    route = jnp.where(lane // 8 == first // 8, turned, 0.0).astype(BF16)
    x = x_ref[...]
    v = x.astype(F32)
    scaled = v * lax.rsqrt(jnp.mean(v * v, axis=-1, keepdims=True) + EPS)
    normed = (scaled * gain[...].astype(F32).reshape(1, D)).astype(BF16)
    for j in range(16):
        at = slice(j * 128, (j + 1) * 128)
        sent[j, 0:16, :] = normed[:, at]
        sent[j, 16:24, :] = half[:, at]
        sent[j, 24:32, :] = route


def prepare(x, gain, ids, shares, ws):
    return pl.pallas_call(
        prepare_body,
        out_shape=[
            jax.ShapeDtypeStruct((16, 32, 128), BF16),
            jax.ShapeDtypeStruct((4, 32, 768), BF16),
        ],
        scratch_shapes=[pltpu.VMEM((8, 128), F32)],
        name="prepare",
    )(x, gain, ids, shares, *ws)


def project_body(x_ref, c0, c1, c2, c3, out_ref, wide, out, sems):
    xi = lax.axis_index("x")
    x = x_ref[:, 0:16, :].reshape(256, 128)
    stores = []
    for p in range(4):
        for offset, chunk in zip(OFFSETS, (c0, c1, c2, c3)):
            at = pl.multiple_of(((xi + offset) % 4) * 32, 32)
            wide[p, pl.ds(at, 32), :] = chunk[p]
        at = pl.ds(p * 768, 768)
        out[:, :, at] = (
            jnp.dot(x, wide[p], preferred_element_type=F32).astype(BF16).reshape(16, 16, 768)
        )
        stores.append(pltpu.make_async_copy(out.at[:, :, at], out_ref.at[:, :, at], sems.at[p]))
        stores[-1].start()
    for store in stores:
        store.wait()


def project(got, chunks):
    return pl.pallas_call(
        project_body,
        in_specs=[VMEM] * 5,
        out_specs=HBM,
        out_shape=jax.ShapeDtypeStruct((16, 16, 3072), BF16),
        scratch_shapes=[
            pltpu.VMEM((4, 128, 768), BF16),
            pltpu.VMEM((16, 16, 3072), BF16),
            pltpu.SemaphoreType.DMA((4,)),
        ],
        compiler_params=pltpu.CompilerParams(vmem_limit_bytes=12 * 2**20),
        name="project",
    )(got, *chunks)


PER_STEP = 2
STEPS = 16 // PER_STEP
FREQUENCY = np.tile(10000.0 ** (-np.arange(64) * 2.0 / 128), 2).astype(np.float32)
TURN = np.repeat([-1.0, 1.0], 64).astype(np.float32)
GAMMA = [float(np.exp(np.log1p(-(2.0 ** (-5.0 - 5.0 * h / (HEADS - 1)))))) for h in range(HEADS)]


def gammas():
    upper = lax.axis_index("tp") == 1
    return [jnp.where(upper, GAMMA[h + 6], GAMMA[h]).astype(F32) for h in range(6)]


def as_columns(row):
    return jnp.transpose(jnp.broadcast_to(row, (128, 128)))


def some_rows(i):
    return pl.ds(i * PER_STEP, PER_STEP)


def recall_body(
    parts, cosine_ref, sine_ref, gain, state_ref, sent, keys, values,
    buf, turns, queries, gates, readouts, sems,
):
    fetch_turns = [
        pltpu.make_async_copy(cosine_ref, turns.at[0], sems.at[STEPS]),
        pltpu.make_async_copy(sine_ref, turns.at[1], sems.at[STEPS + 1]),
    ]
    for c in fetch_turns:
        c.start()

    def fetch(i):
        return pltpu.make_async_copy(
            state_ref.at[some_rows(i)], buf.at[some_rows(i)], sems.at[i]
        )

    for i in range(STEPS):
        fetch(i).start()
    gamma = gammas()
    for c in fetch_turns:
        c.wait()
    cos_v, sin_v = turns[0], turns[1]
    keys[...] = jnp.zeros((16, 8, 128), F32)
    values[...] = jnp.zeros((16, 8, 128), F32)
    added = []
    for h in range(6):
        def total(which):
            at = which * 768 + h * 128
            acc = parts[0, :, at : at + 128].astype(F32)
            for s in range(1, 16):
                acc = acc + parts[s, :, at : at + 128].astype(F32)
            return acc.astype(BF16).astype(F32)

        q, k, v, g = (total(i) for i in range(4))
        query = q * cos_v + pltpu.roll(q, 64, 1) * sin_v
        key = (k * cos_v + pltpu.roll(k, 64, 1) * sin_v) * (128.0 ** -0.5)
        queries[:, h, :] = gamma[h] * query
        keys[:, h, :] = key
        values[:, h, :] = v
        added.append(jnp.sum(query * key, axis=-1, keepdims=True) * v)
        gates[:, h * 128 : (h + 1) * 128] = g * jax.nn.sigmoid(g)

    def some(i, carry):
        fetch(i).wait()
        for j in range(PER_STEP):
            t = i * PER_STEP + j
            for h in range(6):
                q_full = as_columns(queries[t, h : h + 1, :])
                readouts[t, h : h + 1, :] = jnp.sum(q_full * buf[t, h], axis=0, keepdims=True)
        return carry

    lax.fori_loop(0, STEPS, some, 0)
    gains = gain[...].astype(F32).reshape(1, 768)
    for h in range(6):
        at = slice(h * 128, (h + 1) * 128)
        r = readouts[:, h, :] + added[h]
        centred = r - jnp.mean(r, axis=-1, keepdims=True)
        unit = centred * lax.rsqrt(jnp.mean(centred * centred, axis=-1, keepdims=True) + EPS)
        kept = (unit * gains[:, at] * gates[:, at]).astype(BF16)
        for s in range(16):
            sent[s, :, at] = kept


def recall(parts, cosine, sine, gain, state):
    return pl.pallas_call(
        recall_body,
        in_specs=[VMEM, HBM, HBM, VMEM, HBM],
        out_specs=[VMEM] * 3,
        out_shape=[
            jax.ShapeDtypeStruct((16, 16, 768), BF16),
            jax.ShapeDtypeStruct((16, 8, 128), F32),
            jax.ShapeDtypeStruct((16, 8, 128), F32),
        ],
        scratch_shapes=[
            pltpu.VMEM((16, 6, 128, 128), F32),
            pltpu.VMEM((2, 16, 128), F32),
            pltpu.VMEM((16, 8, 128), F32),
            pltpu.VMEM((16, 768), F32),
            pltpu.VMEM((16, 8, 128), F32),
            pltpu.SemaphoreType.DMA((STEPS + 2,)),
        ],
        compiler_params=pltpu.CompilerParams(vmem_limit_bytes=57 * 2**20),
        name="recall",
    )(parts, cosine, sine, gain, state)


def renew_body(keys, values, state_ref, new_state, buf, sems):
    def fetch(i):
        return pltpu.make_async_copy(
            state_ref.at[some_rows(i)], buf.at[some_rows(i)], sems.at[i]
        )

    def store(i):
        return pltpu.make_async_copy(
            buf.at[some_rows(i)], new_state.at[some_rows(i)], sems.at[STEPS + i]
        )

    for i in range(STEPS):
        fetch(i).start()
    gamma = gammas()

    def some(i, carry):
        fetch(i).wait()
        for j in range(PER_STEP):
            t = i * PER_STEP + j
            for h in range(6):
                k_full = as_columns(keys[t, h : h + 1, :])
                buf[t, h] = gamma[h] * buf[t, h] + k_full * values[t, h : h + 1, :]
        store(i).start()
        return carry

    lax.fori_loop(0, STEPS, some, 0)
    for i in range(STEPS):
        store(i).wait()


def renew(keys, values, state):
    return pl.pallas_call(
        renew_body,
        in_specs=[VMEM, VMEM, HBM],
        out_specs=HBM,
        out_shape=jax.ShapeDtypeStruct((16, 6, 128, 128), F32),
        scratch_shapes=[
            pltpu.VMEM((16, 6, 128, 128), F32),
            pltpu.SemaphoreType.DMA((2 * STEPS,)),
        ],
        compiler_params=pltpu.CompilerParams(vmem_limit_bytes=57 * 2**20),
        name="renew",
    )(keys, values, state)


def mix_body(kept, c0, c1, c2, c3, keep, give, wide, mixed):
    xi = lax.axis_index("x")
    core = lax.axis_index("tp")
    for offset, chunk in zip(OFFSETS, (c0, c1, c2, c3)):
        at = pl.multiple_of(((xi + offset) % 4) * 32, 32)
        wide[pl.ds(at, 32), :] = chunk[...]
    rows = kept[...].reshape(256, 768)
    out = lax.dot_general(rows, wide[...], NT, preferred_element_type=F32)
    mixed[...] = out.reshape(16, 16, 128)
    keep[...] = mixed[:, pl.ds(pl.multiple_of(core * 8, 8), 8), :].astype(BF16)
    give[...] = mixed[:, pl.ds(pl.multiple_of((1 - core) * 8, 8), 8), :].astype(BF16)


def mix(kept, chunks):
    half = jax.ShapeDtypeStruct((16, 8, 128), BF16)
    return pl.pallas_call(
        mix_body,
        in_specs=[VMEM] * 5,
        out_shape=[half, half],
        scratch_shapes=[pltpu.VMEM((128, 768), BF16), pltpu.VMEM((16, 16, 128), F32)],
        compiler_params=pltpu.CompilerParams(vmem_limit_bytes=6 * 2**20),
        name="mix",
    )(kept, *chunks)


def settle_body(mine, other, got, out_ref):
    mixer_out = (mine[...].astype(F32) + other[...].astype(F32)).astype(BF16)
    res = (got[:, 16:24, :].astype(F32) + mixer_out.astype(F32)).astype(BF16).reshape(128, 128)
    for s in range(16):
        out_ref[s] = res


def settle(mine, other, got):
    return pl.pallas_call(
        settle_body,
        out_shape=jax.ShapeDtypeStruct((16, 128, 128), BF16),
        compiler_params=pltpu.CompilerParams(vmem_limit_bytes=4 * 2**20),
        name="settle",
    )(mine, other, got)


def spread_body(res, gain, branch, pick, plane, s0, s1, s2, s3, opening, own):
    total = jnp.zeros((128, 128), F32)
    for s in range(16):
        r = res[s].astype(F32)
        total = total + r * r
    scale = lax.rsqrt(jnp.sum(total, axis=-1, keepdims=True) / D + EPS)
    first = pl.multiple_of(lax.axis_index(PLANE) * 8, 8)
    gains = gain[...].astype(F32).reshape(1, D)
    branches = branch[...].astype(F32).reshape(1, D)
    dots = jnp.zeros((128, 128), F32)
    for s in range(16):
        at = slice(s * 128, (s + 1) * 128)
        n = (res[s].astype(F32) * scale * gains[:, at]).astype(BF16)
        plane[:, at] = n
        dots = dots + n.astype(F32) * branches[:, at]
        rows = jnp.dot(pick[...], n, preferred_element_type=F32).astype(BF16)
        for k, out in enumerate((s0, s1, s2, s3)):
            out[:, at] = rows[k * 32 : (k + 1) * 32]
        own[:, at] = res[s, pl.ds(first, 8), :]
    opening[...] = jax.nn.sigmoid(jnp.sum(dots, axis=-1, keepdims=True))


def spread(res, gain, branch, pick):
    rows = jax.ShapeDtypeStruct((32, D), BF16)
    return pl.pallas_call(
        spread_body,
        in_specs=[VMEM] * 4,
        out_shape=[
            jax.ShapeDtypeStruct((128, D), BF16), rows, rows, rows, rows,
            jax.ShapeDtypeStruct((128, 1), F32),
            jax.ShapeDtypeStruct((8, D), BF16),
        ],
        compiler_params=pltpu.CompilerParams(vmem_limit_bytes=10 * 2**20),
        name="spread",
    )(res, gain, branch, pick)


def dense_body(plane, c0, c1, c2, c3, c4, c5, c6, c7, hidden, gate, up):
    for r, chunk in enumerate((c0, c1, c2, c3, c4, c5, c6, c7)):
        at = slice(r * 32, (r + 1) * 32)
        gate[at, :] = chunk[0:32, :]
        up[at, :] = chunk[32:64, :]
    x = plane[...]
    g = lax.dot_general(x, gate[...], NT, preferred_element_type=F32)
    u = lax.dot_general(x, up[...], NT, preferred_element_type=F32)
    hidden[...] = (g * jax.nn.sigmoid(g) * u).astype(BF16)


def dense_first(plane, chunks):
    return pl.pallas_call(
        dense_body,
        out_shape=jax.ShapeDtypeStruct((128, 256), BF16),
        scratch_shapes=[pltpu.VMEM((256, D), BF16), pltpu.VMEM((256, D), BF16)],
        compiler_params=pltpu.CompilerParams(vmem_limit_bytes=12 * 2**20),
        name="dense_first",
    )(plane, *chunks)


def expert_body(
    a0, a1, a2, a3, gate_a, gate_b, up_a, up_b, down_a, down_b, r0, r1, r2, r3, rows
):
    for k, a in enumerate((a0, a1, a2, a3)):
        rows[k * 32 : (k + 1) * 32, :] = a[...]
    hidden = []
    for gate, up in ((gate_a, up_a), (gate_b, up_b)):
        g = jnp.dot(rows[...], gate[0], preferred_element_type=F32)
        u = jnp.dot(rows[...], up[0], preferred_element_type=F32)
        hidden.append((g * jax.nn.sigmoid(g) * u).astype(BF16))
    for j in range(4):
        at = slice(j * 512, (j + 1) * 512)
        out = jnp.dot(hidden[0], down_a[0, :, at], preferred_element_type=F32)
        out = (out + jnp.dot(hidden[1], down_b[0, :, at], preferred_element_type=F32)).astype(BF16)
        for k, r in enumerate((r0, r1, r2, r3)):
            r[:, at] = out[k * 32 : (k + 1) * 32, :]


def experts(arrived, weights):
    rows = jax.ShapeDtypeStruct((32, D), BF16)
    return pl.pallas_call(
        expert_body,
        in_specs=[VMEM] * 10,
        out_shape=[rows] * 4,
        scratch_shapes=[pltpu.VMEM((128, D), BF16)],
        compiler_params=pltpu.CompilerParams(vmem_limit_bytes=24 * 2**20),
        name="experts",
    )(*arrived, *weights)


def combine_body(
    hidden, c0, c1, c2, c3, c4, c5, c6, c7, opening, weigh, b0, b1, b2, b3, out, down, back
):
    for r, chunk in enumerate((c0, c1, c2, c3, c4, c5, c6, c7)):
        down[r * 32 : (r + 1) * 32, :] = chunk[64:96, :]
    for k, b in enumerate((b0, b1, b2, b3)):
        back[k * 32 : (k + 1) * 32, :] = b[...]
        back[128 + k * 32 : 128 + (k + 1) * 32, :] = b[...]
    opened = opening[...]
    for j in range(4):
        at = slice(j * 512, (j + 1) * 512)
        term = jnp.dot(hidden[...], down[:, at], preferred_element_type=F32) * opened
        term = term + lax.dot_general(weigh[...], back[:, at], TN, preferred_element_type=F32)
        out[:, :, at] = term.astype(BF16).reshape(16, 8, 512)


def combine(hidden, chunks, opening, weigh, back):
    return pl.pallas_call(
        combine_body,
        out_shape=jax.ShapeDtypeStruct((16, 8, D), BF16),
        scratch_shapes=[pltpu.VMEM((256, D), BF16), pltpu.VMEM((256, D), BF16)],
        compiler_params=pltpu.CompilerParams(vmem_limit_bytes=12 * 2**20),
        name="combine",
    )(hidden, *chunks, opening, weigh, *back)


def hoist_body(*refs):
    n = len(refs) // 2
    ins, outs, sems = refs[:n], refs[n : 2 * n], refs[2 * n]
    moves = [
        pltpu.make_async_copy(a.at[0, half], b.at[0, half], sems.at[2 * i + j])
        for i, (a, b) in enumerate(zip(ins, outs))
        for j, half in enumerate((pl.ds(0, a.shape[1] // 2), pl.ds(a.shape[1] // 2, a.shape[1] // 2)))
    ]
    for m in moves:
        m.start()
    for m in moves:
        m.wait()


def hoist(*arrays):
    return pl.pallas_call(
        hoist_body,
        in_specs=[HBM] * len(arrays),
        out_specs=[VMEM] * len(arrays),
        out_shape=[jax.ShapeDtypeStruct(a.shape, a.dtype) for a in arrays],
        scratch_shapes=[pltpu.SemaphoreType.DMA((2 * len(arrays),))],
        compiler_params=pltpu.CompilerParams(vmem_limit_bytes=40 * 2**20),
        name="hoist",
    )(*arrays)


def plane_exchange(array):
    return lax.all_to_all(array, PLANE, split_axis=0, concat_axis=0, tiled=True)


def routing_body(got, pick, weigh):
    total = got[0, 24:32, :].astype(F32)
    for s in range(1, 16):
        total = total + got[s, 24:32, :].astype(F32)
    ids, weights = total[0:4], total[4:8]
    share = weights / jnp.sum(weights, axis=0, keepdims=True)
    a = lax.broadcasted_iota(jnp.int32, (128, 128), 0)
    b = lax.broadcasted_iota(jnp.int32, (128, 128), 1)
    before = ((a // 8 == b // 8) & (a < b)).astype(F32).astype(BF16)
    slot = lax.broadcasted_iota(jnp.int32, (32, 128), 0)
    token = lax.broadcasted_iota(jnp.int32, (32, 128), 1)
    mine = slot // 2 == token // 8
    x_at = lax.axis_index("x")
    zy_at = lax.axis_index(PLANE)
    for k in range(4):
        wanted = (zy_at * 4 + (x_at + k) % 4).astype(F32)
        hits = (ids == wanted).astype(F32)
        match = jnp.sum(hits, axis=0, keepdims=True)
        share_of = jnp.sum(hits * share, axis=0, keepdims=True)
        many = jnp.broadcast_to(match, (32, 128))
        rank = jnp.dot(many.astype(BF16), before, preferred_element_type=F32)
        place = mine & (rank == (slot % 2).astype(F32)) & (many > 0)
        at = slice(k * 32, (k + 1) * 32)
        pick[at, :] = jnp.where(place, 1.0, 0.0).astype(BF16)
        value = jnp.where(place, jnp.broadcast_to(share_of, (32, 128)), 0.0)
        high = value.astype(BF16)
        weigh[at, :] = high
        weigh[k * 32 + 128 : k * 32 + 160, :] = (value - high.astype(F32)).astype(BF16)


def routing(got):
    return pl.pallas_call(
        routing_body,
        out_shape=[
            jax.ShapeDtypeStruct((128, 128), BF16),
            jax.ShapeDtypeStruct((256, 128), BF16),
        ],
        compiler_params=pltpu.CompilerParams(vmem_limit_bytes=4 * 2**20),
        name="routing",
    )(got)


def on_device(
    inputs, positions, ret_state, norm_mix, w_query, w_key, w_value, w_gate_in, head_gain, w_out,
    norm_ffn, route_ids, route_weight, exp_gate, exp_up, exp_down, dense_gate, dense_up, dense_down,
    branch_gate,
):
    core = lax.axis_index("tp")

    sent, w4 = prepare(
        inputs, norm_mix, route_ids.T, route_weight.T, (w_query, w_key, w_value, w_gate_in)
    )
    chunks = ring_gather(w4)
    got = plane_exchange(sent)

    angles = positions.astype(F32)[:, None] * FREQUENCY[None, :]
    cosine = jnp.cos(angles)
    sine = jnp.sin(angles) * TURN[None, :]
    dense = jnp.concatenate([dense_gate.T, dense_up.T, dense_down], axis=0)
    partial = project(got, chunks)
    partial, got, cosine, sine, dense = lax.optimization_barrier(
        (partial, got, cosine, sine, dense)
    )
    expert_own = (exp_gate, exp_up, exp_down)
    parts = plane_exchange(partial)

    out_chunks = ring_gather(w_out.T)
    dense_chunks = ring_gather(dense)
    expert_other = tuple(lax.ppermute(w, "tp", SWAP) for w in expert_own)
    dense_chunks = dense_chunks + tuple(lax.ppermute(c, "tp", SWAP) for c in dense_chunks)
    pick, weigh = routing(got)

    kept, keys, values = recall(parts, cosine, sine, head_gain, ret_state)
    kept = plane_exchange(kept)
    kept, out_chunks, dense_chunks, expert_other, pick, weigh = lax.optimization_barrier(
        (kept, out_chunks, dense_chunks, expert_other, pick, weigh)
    )
    keep, give = mix(kept, out_chunks)
    settled = settle(keep, lax.ppermute(give, "tp", SWAP), got)
    res = plane_exchange(settled)
    new_state = renew(keys, values, ret_state)

    plane, s0, s1, s2, s3, opening, own_res = spread(res, norm_ffn, branch_gate, pick)
    arrived = (
        s0,
        lax.ppermute(s1, "x", RIGHT),
        lax.ppermute(s2, "x", ACROSS),
        lax.ppermute(s3, "x", LEFT),
    )
    hidden = dense_first(plane, dense_chunks)
    weights = tuple(w for pair in zip(expert_own, expert_other) for w in pair)
    weights = hoist(*weights)
    r0, r1, r2, r3 = experts(arrived, weights)
    back = (
        r0,
        lax.ppermute(r1, "x", LEFT),
        lax.ppermute(r2, "x", ACROSS),
        lax.ppermute(r3, "x", RIGHT),
    )
    branch = combine(hidden, dense_chunks, opening, weigh, back)
    terms = plane_exchange(branch)
    summed = jnp.sum(terms.astype(F32), axis=0)
    mine = (own_res.astype(F32) + summed).astype(BF16)
    other = lax.ppermute(mine, "tp", SWAP)
    layer_out = jnp.concatenate(
        [jnp.where(core == 0, mine, other), jnp.where(core == 0, other, mine)], axis=0
    )
    return (layer_out, new_state)


EP = ("z", "y", "x")


def solution(mesh):
    inner = Mesh(mesh.devices.reshape(4, 4, 4, 2), ("z", "y", "x", "tp"))
    in_specs = (
        P(EP, None),
        P(EP),
        P(EP, "tp", None, None),
        P(),
        P(EP, "tp"),
        P(EP, "tp"),
        P(EP, "tp"),
        P(EP, "tp"),
        P("tp"),
        P("tp", EP),
        P(),
        P(EP, None),
        P(EP, None),
        P(EP, None, "tp"),
        P(EP, None, "tp"),
        P(EP, "tp", None),
        P(None, (*EP, "tp")),
        P(None, (*EP, "tp")),
        P((*EP, "tp"), None),
        P(),
    )
    out_specs = (P(EP, None), P(EP, "tp", None, None))
    return jax.shard_map(
        on_device, mesh=inner, in_specs=in_specs, out_specs=out_specs, check_vma=False
    )
```

```python
import functools

import jax
import jax.numpy as jnp
import numpy as np
from jax import lax
from jax.experimental import pallas as pl
from jax.experimental.pallas import tpu as pltpu
from jax.sharding import Mesh, PartitionSpec as P


D = 2048
HEADS = 12
EPS = 1e-06
F32 = jnp.float32
BF16 = jnp.bfloat16

RIGHT = [(i, (i + 1) % 4) for i in range(4)]
LEFT = [(i, (i - 1) % 4) for i in range(4)]
ACROSS = [(i, (i + 2) % 4) for i in range(4)]
SWAP = [(0, 1), (1, 0)]
PLANE = ("z", "y")
NT = (((1,), (1,)), ((), ()))
TN = (((0,), (0,)), ((), ()))
HBM = pl.BlockSpec(memory_space=pltpu.HBM)
VMEM = pl.BlockSpec(memory_space=pltpu.VMEM)


def ring_gather(own):
    return (
        own,
        lax.ppermute(own, "x", RIGHT),
        lax.ppermute(own, "x", ACROSS),
        lax.ppermute(own, "x", LEFT),
    )


OFFSETS = (0, 3, 2, 1)


SMEM = pl.BlockSpec(memory_space=pltpu.SMEM)


def prepare_body(x_ref, gain, ids, shares, wq, wk, wv, wg, sent, w4, routes):
    w4[0] = wq[...]
    w4[1] = wk[...]
    w4[2] = wv[...]
    w4[3] = wg[...]
    half = x_ref[pl.ds(pl.multiple_of(lax.axis_index("tp") * 8, 8), 8), :]
    routes[...] = jnp.zeros((8, 128), F32)
    routes[0:4, 0:16] = ids[...].astype(F32)
    routes[4:8, 0:16] = shares[...].astype(F32)
    first = lax.axis_index(PLANE) * 8
    turned = pltpu.roll(routes[...], (first - lax.axis_index("tp") * 8 + 128) % 128, 1)
    lane = lax.broadcasted_iota(jnp.int32, (8, 128), 1)
    route = jnp.where(lane // 8 == first // 8, turned, 0.0).astype(BF16)
    x = x_ref[...]
    v = x.astype(F32)
    scaled = v * lax.rsqrt(jnp.mean(v * v, axis=-1, keepdims=True) + EPS)
    normed = (scaled * gain[...].astype(F32).reshape(1, D)).astype(BF16)
    for j in range(16):
        at = slice(j * 128, (j + 1) * 128)
        sent[j, 0:16, :] = normed[:, at]
        sent[j, 16:24, :] = half[:, at]
        sent[j, 24:32, :] = route


def prepare(x, gain, ids, shares, ws):
    return pl.pallas_call(
        prepare_body,
        out_shape=[
            jax.ShapeDtypeStruct((16, 32, 128), BF16),
            jax.ShapeDtypeStruct((4, 32, 768), BF16),
        ],
        scratch_shapes=[pltpu.VMEM((8, 128), F32)],
        name="prepare",
    )(x, gain, ids, shares, *ws)


def project_body(x_ref, c0, c1, c2, c3, out_ref, wide, out, sems):
    xi = lax.axis_index("x")
    x = x_ref[:, 0:16, :].reshape(256, 128)
    stores = []
    for p in range(4):
        for offset, chunk in zip(OFFSETS, (c0, c1, c2, c3)):
            at = pl.multiple_of(((xi + offset) % 4) * 32, 32)
            wide[p, pl.ds(at, 32), :] = chunk[p]
        at = pl.ds(p * 768, 768)
        out[:, :, at] = (
            jnp.dot(x, wide[p], preferred_element_type=F32).astype(BF16).reshape(16, 16, 768)
        )
        stores.append(pltpu.make_async_copy(out.at[:, :, at], out_ref.at[:, :, at], sems.at[p]))
        stores[-1].start()
    for store in stores:
        store.wait()


def project(got, chunks):
    return pl.pallas_call(
        project_body,
        in_specs=[VMEM] * 5,
        out_specs=HBM,
        out_shape=jax.ShapeDtypeStruct((16, 16, 3072), BF16),
        scratch_shapes=[
            pltpu.VMEM((4, 128, 768), BF16),
            pltpu.VMEM((16, 16, 3072), BF16),
            pltpu.SemaphoreType.DMA((4,)),
        ],
        compiler_params=pltpu.CompilerParams(vmem_limit_bytes=12 * 2**20),
        name="project",
    )(got, *chunks)


PER_STEP = 2
STEPS = 16 // PER_STEP
AHEAD = 8
FREQUENCY = np.tile(10000.0 ** (-np.arange(64) * 2.0 / 128), 2).astype(np.float32)
TURN = np.repeat([-1.0, 1.0], 64).astype(np.float32)
GAMMA = [float(np.exp(np.log1p(-(2.0 ** (-5.0 - 5.0 * h / (HEADS - 1)))))) for h in range(HEADS)]


def gammas():
    upper = lax.axis_index("tp") == 1
    return [jnp.where(upper, GAMMA[h + 6], GAMMA[h]).astype(F32) for h in range(6)]


def as_columns(row):
    return jnp.transpose(jnp.broadcast_to(row, (128, 128)))


def some_rows(i):
    return pl.ds(i * PER_STEP, PER_STEP)


def recall_body(
    parts, cosine_ref, sine_ref, gain, state_ref, sent, keys, values,
    buf, turns, queries, gates, readouts, sems,
):
    fetch_turns = [
        pltpu.make_async_copy(cosine_ref, turns.at[0], sems.at[STEPS]),
        pltpu.make_async_copy(sine_ref, turns.at[1], sems.at[STEPS + 1]),
    ]
    for c in fetch_turns:
        c.start()

    def fetch(i):
        return pltpu.make_async_copy(
            state_ref.at[some_rows(i)], buf.at[some_rows(i)], sems.at[i]
        )

    for i in range(AHEAD):
        fetch(i).start()
    gamma = gammas()
    for c in fetch_turns:
        c.wait()
    cos_v, sin_v = turns[0], turns[1]
    keys[...] = jnp.zeros((16, 8, 128), F32)
    values[...] = jnp.zeros((16, 8, 128), F32)
    added = []
    for h in range(6):
        def total(which):
            at = which * 768 + h * 128
            acc = parts[0, :, at : at + 128].astype(F32)
            for s in range(1, 16):
                acc = acc + parts[s, :, at : at + 128].astype(F32)
            return acc.astype(BF16).astype(F32)

        q, k, v, g = (total(i) for i in range(4))
        query = q * cos_v + pltpu.roll(q, 64, 1) * sin_v
        key = (k * cos_v + pltpu.roll(k, 64, 1) * sin_v) * (128.0 ** -0.5)
        queries[:, h, :] = gamma[h] * query
        keys[:, h, :] = key
        values[:, h, :] = v
        added.append(jnp.sum(query * key, axis=-1, keepdims=True) * v)
        gates[:, h * 128 : (h + 1) * 128] = g * jax.nn.sigmoid(g)

    def some(i, carry):
        fetch(i).wait()

        @pl.when(i + AHEAD < STEPS)
        def _():
            fetch(i + AHEAD).start()

        for j in range(PER_STEP):
            t = i * PER_STEP + j
            for h in range(6):
                q_full = as_columns(queries[t, h : h + 1, :])
                readouts[t, h : h + 1, :] = jnp.sum(q_full * buf[t, h], axis=0, keepdims=True)
        return carry

    lax.fori_loop(0, STEPS, some, 0)
    gains = gain[...].astype(F32).reshape(1, 768)
    for h in range(6):
        at = slice(h * 128, (h + 1) * 128)
        r = readouts[:, h, :] + added[h]
        centred = r - jnp.mean(r, axis=-1, keepdims=True)
        unit = centred * lax.rsqrt(jnp.mean(centred * centred, axis=-1, keepdims=True) + EPS)
        kept = (unit * gains[:, at] * gates[:, at]).astype(BF16)
        for s in range(16):
            sent[s, :, at] = kept


def recall(parts, cosine, sine, gain, state):
    return pl.pallas_call(
        recall_body,
        in_specs=[VMEM, HBM, HBM, VMEM, HBM],
        out_specs=[VMEM] * 3,
        out_shape=[
            jax.ShapeDtypeStruct((16, 16, 768), BF16),
            jax.ShapeDtypeStruct((16, 8, 128), F32),
            jax.ShapeDtypeStruct((16, 8, 128), F32),
        ],
        scratch_shapes=[
            pltpu.VMEM((16, 6, 128, 128), F32),
            pltpu.VMEM((2, 16, 128), F32),
            pltpu.VMEM((16, 8, 128), F32),
            pltpu.VMEM((16, 768), F32),
            pltpu.VMEM((16, 8, 128), F32),
            pltpu.SemaphoreType.DMA((STEPS + 2,)),
        ],
        compiler_params=pltpu.CompilerParams(vmem_limit_bytes=57 * 2**20),
        name="recall",
    )(parts, cosine, sine, gain, state)


def renew_body(first, keys, values, state_ref, *rest):
    new_state, buf, sems = rest[-3:]

    def fetch(i):
        return pltpu.make_async_copy(
            state_ref.at[some_rows(first + i)], buf.at[some_rows(i)], sems.at[i]
        )

    def store(i):
        return pltpu.make_async_copy(
            buf.at[some_rows(i)], new_state.at[some_rows(first + i)], sems.at[HALF + i]
        )

    for i in range(HALF):
        fetch(i).start()
    gamma = gammas()

    def some(i, carry):
        fetch(i).wait()
        for j in range(PER_STEP):
            t = i * PER_STEP + j
            at = first * PER_STEP + t
            for h in range(6):
                k_full = as_columns(keys[at, h : h + 1, :])
                buf[t, h] = gamma[h] * buf[t, h] + k_full * values[at, h : h + 1, :]
        store(i).start()
        return carry

    lax.fori_loop(0, HALF, some, 0)
    for i in range(HALF):
        store(i).wait()


HALF = STEPS // 2


def renew(keys, values, state, half, *before):
    return pl.pallas_call(
        functools.partial(renew_body, half * HALF),
        in_specs=[VMEM, VMEM, HBM] + [HBM] * len(before),
        out_specs=HBM,
        out_shape=jax.ShapeDtypeStruct((16, 6, 128, 128), F32),
        input_output_aliases={3: 0} if before else {},
        scratch_shapes=[
            pltpu.VMEM((16 // 2, 6, 128, 128), F32),
            pltpu.SemaphoreType.DMA((2 * HALF,)),
        ],
        compiler_params=pltpu.CompilerParams(vmem_limit_bytes=57 * 2**20),
    )(keys, values, state, *before)


def mix_body(kept, c0, c1, c2, c3, keep, give, wide, mixed):
    xi = lax.axis_index("x")
    core = lax.axis_index("tp")
    for offset, chunk in zip(OFFSETS, (c0, c1, c2, c3)):
        at = pl.multiple_of(((xi + offset) % 4) * 32, 32)
        wide[pl.ds(at, 32), :] = chunk[...]
    rows = kept[...].reshape(256, 768)
    out = lax.dot_general(rows, wide[...], NT, preferred_element_type=F32)
    mixed[...] = out.reshape(16, 16, 128)
    keep[...] = mixed[:, pl.ds(pl.multiple_of(core * 8, 8), 8), :].astype(BF16)
    give[...] = mixed[:, pl.ds(pl.multiple_of((1 - core) * 8, 8), 8), :].astype(BF16)


def mix(kept, chunks):
    half = jax.ShapeDtypeStruct((16, 8, 128), BF16)
    return pl.pallas_call(
        mix_body,
        in_specs=[VMEM] * 5,
        out_shape=[half, half],
        scratch_shapes=[pltpu.VMEM((128, 768), BF16), pltpu.VMEM((16, 16, 128), F32)],
        compiler_params=pltpu.CompilerParams(vmem_limit_bytes=6 * 2**20),
        name="mix",
    )(kept, *chunks)


def settle_body(mine, other, got, out_ref):
    mixer_out = (mine[...].astype(F32) + other[...].astype(F32)).astype(BF16)
    res = (got[:, 16:24, :].astype(F32) + mixer_out.astype(F32)).astype(BF16).reshape(128, 128)
    for s in range(16):
        out_ref[s] = res


def settle(mine, other, got):
    return pl.pallas_call(
        settle_body,
        out_shape=jax.ShapeDtypeStruct((16, 128, 128), BF16),
        compiler_params=pltpu.CompilerParams(vmem_limit_bytes=4 * 2**20),
        name="settle",
    )(mine, other, got)


def spread_body(res, gain, branch, pick, plane, s0, s1, s2, s3, opening, own):
    total = jnp.zeros((128, 128), F32)
    for s in range(16):
        r = res[s].astype(F32)
        total = total + r * r
    scale = lax.rsqrt(jnp.sum(total, axis=-1, keepdims=True) / D + EPS)
    first = pl.multiple_of(lax.axis_index(PLANE) * 8, 8)
    gains = gain[...].astype(F32).reshape(1, D)
    branches = branch[...].astype(F32).reshape(1, D)
    dots = jnp.zeros((128, 128), F32)
    for s in range(16):
        at = slice(s * 128, (s + 1) * 128)
        n = (res[s].astype(F32) * scale * gains[:, at]).astype(BF16)
        plane[:, at] = n
        dots = dots + n.astype(F32) * branches[:, at]
        rows = jnp.dot(pick[...], n, preferred_element_type=F32).astype(BF16)
        for k, out in enumerate((s0, s1, s2, s3)):
            out[:, at] = rows[k * 32 : (k + 1) * 32]
        own[:, at] = res[s, pl.ds(first, 8), :]
    opening[...] = jax.nn.sigmoid(jnp.sum(dots, axis=-1, keepdims=True))


def spread(res, gain, branch, pick):
    rows = jax.ShapeDtypeStruct((32, D), BF16)
    return pl.pallas_call(
        spread_body,
        in_specs=[VMEM] * 4,
        out_shape=[
            jax.ShapeDtypeStruct((128, D), BF16), rows, rows, rows, rows,
            jax.ShapeDtypeStruct((128, 1), F32),
            jax.ShapeDtypeStruct((8, D), BF16),
        ],
        compiler_params=pltpu.CompilerParams(vmem_limit_bytes=10 * 2**20),
        name="spread",
    )(res, gain, branch, pick)


def dense_body(plane, c0, c1, c2, c3, c4, c5, c6, c7, hidden, down, gate, up):
    for r, chunk in enumerate((c0, c1, c2, c3, c4, c5, c6, c7)):
        at = slice(r * 32, (r + 1) * 32)
        gate[at, :] = chunk[0:32, :]
        up[at, :] = chunk[32:64, :]
        down[at, :] = chunk[64:96, :]
    x = plane[...]
    g = lax.dot_general(x, gate[...], NT, preferred_element_type=F32)
    u = lax.dot_general(x, up[...], NT, preferred_element_type=F32)
    hidden[...] = (g * jax.nn.sigmoid(g) * u).astype(BF16)


def dense_first(plane, chunks):
    return pl.pallas_call(
        dense_body,
        out_shape=[
            jax.ShapeDtypeStruct((128, 256), BF16),
            jax.ShapeDtypeStruct((256, D), BF16),
        ],
        scratch_shapes=[pltpu.VMEM((256, D), BF16), pltpu.VMEM((256, D), BF16)],
        compiler_params=pltpu.CompilerParams(vmem_limit_bytes=12 * 2**20),
        name="dense_first",
    )(plane, *chunks)


def expert_body(
    a0, a1, a2, a3, gate_a, gate_b, up_a, up_b, down_a, down_b, r0, r1, r2, r3, rows
):
    for k, a in enumerate((a0, a1, a2, a3)):
        rows[k * 32 : (k + 1) * 32, :] = a[...]
    hidden = []
    for gate, up in ((gate_a, up_a), (gate_b, up_b)):
        g = jnp.dot(rows[...], gate[0], preferred_element_type=F32)
        u = jnp.dot(rows[...], up[0], preferred_element_type=F32)
        hidden.append((g * jax.nn.sigmoid(g) * u).astype(BF16))
    for j in range(4):
        at = slice(j * 512, (j + 1) * 512)
        out = jnp.dot(hidden[0], down_a[0, :, at], preferred_element_type=F32)
        out = (out + jnp.dot(hidden[1], down_b[0, :, at], preferred_element_type=F32)).astype(BF16)
        for k, r in enumerate((r0, r1, r2, r3)):
            r[:, at] = out[k * 32 : (k + 1) * 32, :]


def experts(arrived, weights):
    rows = jax.ShapeDtypeStruct((32, D), BF16)
    return pl.pallas_call(
        expert_body,
        in_specs=[VMEM] * 10,
        out_shape=[rows] * 4,
        scratch_shapes=[pltpu.VMEM((128, D), BF16)],
        compiler_params=pltpu.CompilerParams(vmem_limit_bytes=24 * 2**20),
        name="experts",
    )(*arrived, *weights)


def combine_body(hidden, down, opening, weigh, b0, b1, b2, b3, out, back):
    for k, b in enumerate((b0, b1, b2, b3)):
        back[k * 32 : (k + 1) * 32, :] = b[...]
        back[128 + k * 32 : 128 + (k + 1) * 32, :] = b[...]
    opened = opening[...]
    for j in range(4):
        at = slice(j * 512, (j + 1) * 512)
        term = jnp.dot(hidden[...], down[:, at], preferred_element_type=F32) * opened
        term = term + lax.dot_general(weigh[...], back[:, at], TN, preferred_element_type=F32)
        out[:, :, at] = term.astype(BF16).reshape(16, 8, 512)


def combine(hidden, down, opening, weigh, back):
    return pl.pallas_call(
        combine_body,
        out_shape=jax.ShapeDtypeStruct((16, 8, D), BF16),
        scratch_shapes=[pltpu.VMEM((256, D), BF16)],
        compiler_params=pltpu.CompilerParams(vmem_limit_bytes=12 * 2**20),
        name="combine",
    )(hidden, down, opening, weigh, *back)


def hoist_body(*refs):
    n = len(refs) // 2
    ins, outs, sems = refs[:n], refs[n : 2 * n], refs[2 * n]
    moves = [
        pltpu.make_async_copy(a.at[0, half], b.at[0, half], sems.at[2 * i + j])
        for i, (a, b) in enumerate(zip(ins, outs))
        for j, half in enumerate((pl.ds(0, a.shape[1] // 2), pl.ds(a.shape[1] // 2, a.shape[1] // 2)))
    ]
    for m in moves:
        m.start()
    for m in moves:
        m.wait()


def hoist(*arrays):
    return pl.pallas_call(
        hoist_body,
        in_specs=[HBM] * len(arrays),
        out_specs=[VMEM] * len(arrays),
        out_shape=[jax.ShapeDtypeStruct(a.shape, a.dtype) for a in arrays],
        scratch_shapes=[pltpu.SemaphoreType.DMA((2 * len(arrays),))],
        compiler_params=pltpu.CompilerParams(vmem_limit_bytes=40 * 2**20),
        name="hoist",
    )(*arrays)


def plane_exchange(array):
    return lax.all_to_all(array, PLANE, split_axis=0, concat_axis=0, tiled=True)


def routing_body(got, pick, weigh):
    total = got[0, 24:32, :].astype(F32)
    for s in range(1, 16):
        total = total + got[s, 24:32, :].astype(F32)
    ids, weights = total[0:4], total[4:8]
    share = weights / jnp.sum(weights, axis=0, keepdims=True)
    a = lax.broadcasted_iota(jnp.int32, (128, 128), 0)
    b = lax.broadcasted_iota(jnp.int32, (128, 128), 1)
    before = ((a // 8 == b // 8) & (a < b)).astype(F32).astype(BF16)
    slot = lax.broadcasted_iota(jnp.int32, (32, 128), 0)
    token = lax.broadcasted_iota(jnp.int32, (32, 128), 1)
    mine = slot // 2 == token // 8
    x_at = lax.axis_index("x")
    zy_at = lax.axis_index(PLANE)
    for k in range(4):
        wanted = (zy_at * 4 + (x_at + k) % 4).astype(F32)
        hits = (ids == wanted).astype(F32)
        match = jnp.sum(hits, axis=0, keepdims=True)
        share_of = jnp.sum(hits * share, axis=0, keepdims=True)
        many = jnp.broadcast_to(match, (32, 128))
        rank = jnp.dot(many.astype(BF16), before, preferred_element_type=F32)
        place = mine & (rank == (slot % 2).astype(F32)) & (many > 0)
        at = slice(k * 32, (k + 1) * 32)
        pick[at, :] = jnp.where(place, 1.0, 0.0).astype(BF16)
        value = jnp.where(place, jnp.broadcast_to(share_of, (32, 128)), 0.0)
        high = value.astype(BF16)
        weigh[at, :] = high
        weigh[k * 32 + 128 : k * 32 + 160, :] = (value - high.astype(F32)).astype(BF16)


def routing(got):
    return pl.pallas_call(
        routing_body,
        out_shape=[
            jax.ShapeDtypeStruct((128, 128), BF16),
            jax.ShapeDtypeStruct((256, 128), BF16),
        ],
        compiler_params=pltpu.CompilerParams(vmem_limit_bytes=4 * 2**20),
        name="routing",
    )(got)


def on_device(
    inputs, positions, ret_state, norm_mix, w_query, w_key, w_value, w_gate_in, head_gain, w_out,
    norm_ffn, route_ids, route_weight, exp_gate, exp_up, exp_down, dense_gate, dense_up, dense_down,
    branch_gate,
):
    core = lax.axis_index("tp")

    sent, w4 = prepare(
        inputs, norm_mix, route_ids.T, route_weight.T, (w_query, w_key, w_value, w_gate_in)
    )
    chunks = ring_gather(w4)
    got = plane_exchange(sent)

    partial = project(got, chunks)
    partial, positions, dense_gate, dense_up, dense_down = lax.optimization_barrier(
        (partial, positions, dense_gate, dense_up, dense_down)
    )
    angles = positions.astype(F32)[:, None] * FREQUENCY[None, :]
    cosine = jnp.cos(angles)
    sine = jnp.sin(angles) * TURN[None, :]
    dense = jnp.concatenate([dense_gate.T, dense_up.T, dense_down], axis=0)
    expert_own = (exp_gate, exp_up, exp_down)
    parts = plane_exchange(partial)

    out_chunks = ring_gather(w_out.T)
    dense_chunks = ring_gather(dense)
    expert_other = tuple(lax.ppermute(w, "tp", SWAP) for w in expert_own)
    kept, keys, values = recall(parts, cosine, sine, head_gain, ret_state)
    kept = plane_exchange(kept)
    pick, weigh = routing(got)
    kept, out_chunks, dense_chunks, expert_other = lax.optimization_barrier(
        (kept, out_chunks, dense_chunks, expert_other)
    )
    dense_chunks = dense_chunks + tuple(lax.ppermute(c, "tp", SWAP) for c in dense_chunks)

    keep, give = mix(kept, out_chunks)
    settled = settle(keep, lax.ppermute(give, "tp", SWAP), got)
    res = plane_exchange(settled)
    new_state = renew(keys, values, ret_state, 0)

    plane, s0, s1, s2, s3, opening, own_res = spread(res, norm_ffn, branch_gate, pick)
    arrived = (
        s0,
        lax.ppermute(s1, "x", RIGHT),
        lax.ppermute(s2, "x", ACROSS),
        lax.ppermute(s3, "x", LEFT),
    )
    new_state = renew(keys, values, ret_state, 1, new_state)
    plane, new_state = lax.optimization_barrier((plane, new_state))
    hidden, down = dense_first(plane, dense_chunks)
    weights = tuple(w for pair in zip(expert_own, expert_other) for w in pair)
    weights = hoist(*weights)
    r0, r1, r2, r3 = experts(arrived, weights)
    back = (
        r0,
        lax.ppermute(r1, "x", LEFT),
        lax.ppermute(r2, "x", ACROSS),
        lax.ppermute(r3, "x", RIGHT),
    )
    branch = combine(hidden, down, opening, weigh, back)
    terms = plane_exchange(branch)
    summed = jnp.sum(terms.astype(F32), axis=0)
    mine = (own_res.astype(F32) + summed).astype(BF16)
    other = lax.ppermute(mine, "tp", SWAP)
    layer_out = jnp.concatenate(
        [jnp.where(core == 0, mine, other), jnp.where(core == 0, other, mine)], axis=0
    )
    return (layer_out, new_state)


EP = ("z", "y", "x")


def solution(mesh):
    inner = Mesh(mesh.devices.reshape(4, 4, 4, 2), ("z", "y", "x", "tp"))
    in_specs = (
        P(EP, None),
        P(EP),
        P(EP, "tp", None, None),
        P(),
        P(EP, "tp"),
        P(EP, "tp"),
        P(EP, "tp"),
        P(EP, "tp"),
        P("tp"),
        P("tp", EP),
        P(),
        P(EP, None),
        P(EP, None),
        P(EP, None, "tp"),
        P(EP, None, "tp"),
        P(EP, "tp", None),
        P(None, (*EP, "tp")),
        P(None, (*EP, "tp")),
        P((*EP, "tp"), None),
        P(),
    )
    out_specs = (P(EP, None), P(EP, "tp", None, None))
    return jax.shard_map(
        on_device, mesh=inner, in_specs=in_specs, out_specs=out_specs, check_vma=False
    )
```

```python
import jax
import jax.numpy as jnp
import numpy as np
from jax import lax
from jax.experimental import pallas as pl
from jax.experimental.pallas import tpu as pltpu
from jax.sharding import Mesh, PartitionSpec as P


D = 2048
HEADS = 12
EPS = 1e-06
F32 = jnp.float32
BF16 = jnp.bfloat16

RIGHT = [(i, (i + 1) % 4) for i in range(4)]
LEFT = [(i, (i - 1) % 4) for i in range(4)]
ACROSS = [(i, (i + 2) % 4) for i in range(4)]
SWAP = [(0, 1), (1, 0)]
PLANE = ("z", "y")
NT = (((1,), (1,)), ((), ()))
TN = (((0,), (0,)), ((), ()))
HBM = pl.BlockSpec(memory_space=pltpu.HBM)
VMEM = pl.BlockSpec(memory_space=pltpu.VMEM)


def ring_gather(own):
    return (
        own,
        lax.ppermute(own, "x", RIGHT),
        lax.ppermute(own, "x", ACROSS),
        lax.ppermute(own, "x", LEFT),
    )


OFFSETS = (0, 3, 2, 1)


SMEM = pl.BlockSpec(memory_space=pltpu.SMEM)


def prepare_body(x_ref, gain, ids, shares, wq, wk, wv, wg, sent, w4, routes):
    w4[0] = wq[...]
    w4[1] = wk[...]
    w4[2] = wv[...]
    w4[3] = wg[...]
    half = x_ref[pl.ds(pl.multiple_of(lax.axis_index("tp") * 8, 8), 8), :]
    routes[...] = jnp.zeros((8, 128), F32)
    routes[0:4, 0:16] = ids[...].astype(F32)
    routes[4:8, 0:16] = shares[...].astype(F32)
    first = lax.axis_index(PLANE) * 8
    turned = pltpu.roll(routes[...], (first - lax.axis_index("tp") * 8 + 128) % 128, 1)
    lane = lax.broadcasted_iota(jnp.int32, (8, 128), 1)
    route = jnp.where(lane // 8 == first // 8, turned, 0.0).astype(BF16)
    x = x_ref[...]
    v = x.astype(F32)
    scaled = v * lax.rsqrt(jnp.mean(v * v, axis=-1, keepdims=True) + EPS)
    normed = (scaled * gain[...].astype(F32).reshape(1, D)).astype(BF16)
    for j in range(16):
        at = slice(j * 128, (j + 1) * 128)
        sent[j, 0:16, :] = normed[:, at]
        sent[j, 16:24, :] = half[:, at]
        sent[j, 24:32, :] = route


def prepare(x, gain, ids, shares, ws):
    return pl.pallas_call(
        prepare_body,
        out_shape=[
            jax.ShapeDtypeStruct((16, 32, 128), BF16),
            jax.ShapeDtypeStruct((4, 32, 768), BF16),
        ],
        scratch_shapes=[pltpu.VMEM((8, 128), F32)],
        name="prepare",
    )(x, gain, ids, shares, *ws)


def project_body(x_ref, c0, c1, c2, c3, out_ref, wide, out, sems):
    xi = lax.axis_index("x")
    x = x_ref[:, 0:16, :].reshape(256, 128)
    stores = []
    for p in range(4):
        for offset, chunk in zip(OFFSETS, (c0, c1, c2, c3)):
            at = pl.multiple_of(((xi + offset) % 4) * 32, 32)
            wide[p, pl.ds(at, 32), :] = chunk[p]
        at = pl.ds(p * 768, 768)
        out[:, :, at] = (
            jnp.dot(x, wide[p], preferred_element_type=F32).astype(BF16).reshape(16, 16, 768)
        )
        stores.append(pltpu.make_async_copy(out.at[:, :, at], out_ref.at[:, :, at], sems.at[p]))
        stores[-1].start()
    for store in stores:
        store.wait()


def project(got, chunks):
    return pl.pallas_call(
        project_body,
        in_specs=[VMEM] * 5,
        out_specs=HBM,
        out_shape=jax.ShapeDtypeStruct((16, 16, 3072), BF16),
        scratch_shapes=[
            pltpu.VMEM((4, 128, 768), BF16),
            pltpu.VMEM((16, 16, 3072), BF16),
            pltpu.SemaphoreType.DMA((4,)),
        ],
        compiler_params=pltpu.CompilerParams(vmem_limit_bytes=12 * 2**20),
        name="project",
    )(got, *chunks)


PER_STEP = 4
STEPS = 16 // PER_STEP
AHEAD = 4
FREQUENCY = np.tile(10000.0 ** (-np.arange(64) * 2.0 / 128), 2).astype(np.float32)
TURN = np.repeat([-1.0, 1.0], 64).astype(np.float32)
GAMMA = [float(np.exp(np.log1p(-(2.0 ** (-5.0 - 5.0 * h / (HEADS - 1)))))) for h in range(HEADS)]


def gammas():
    upper = lax.axis_index("tp") == 1
    return [jnp.where(upper, GAMMA[h + 6], GAMMA[h]).astype(F32) for h in range(6)]


def as_columns(row):
    return jnp.transpose(jnp.broadcast_to(row, (128, 128)))


def some_rows(i):
    return pl.ds(i * PER_STEP, PER_STEP)


def recall_body(
    parts, cosine_ref, sine_ref, gain, state_ref, sent, keys, values,
    buf, turns, queries, gates, readouts, sems,
):
    fetch_turns = [
        pltpu.make_async_copy(cosine_ref, turns.at[0], sems.at[STEPS]),
        pltpu.make_async_copy(sine_ref, turns.at[1], sems.at[STEPS + 1]),
    ]
    for c in fetch_turns:
        c.start()

    def fetch(i):
        return pltpu.make_async_copy(
            state_ref.at[some_rows(i)], buf.at[some_rows(i)], sems.at[i]
        )

    for i in range(AHEAD):
        fetch(i).start()
    gamma = gammas()
    for c in fetch_turns:
        c.wait()
    cos_v, sin_v = turns[0], turns[1]
    keys[...] = jnp.zeros((16, 8, 128), F32)
    values[...] = jnp.zeros((16, 8, 128), F32)
    added = []
    for h in range(6):
        def total(which):
            at = which * 768 + h * 128
            acc = parts[0, :, at : at + 128].astype(F32)
            for s in range(1, 16):
                acc = acc + parts[s, :, at : at + 128].astype(F32)
            return acc.astype(BF16).astype(F32)

        q, k, v, g = (total(i) for i in range(4))
        query = q * cos_v + pltpu.roll(q, 64, 1) * sin_v
        key = (k * cos_v + pltpu.roll(k, 64, 1) * sin_v) * (128.0 ** -0.5)
        queries[:, h, :] = gamma[h] * query
        keys[:, h, :] = key
        values[:, h, :] = v
        added.append(jnp.sum(query * key, axis=-1, keepdims=True) * v)
        gates[:, h * 128 : (h + 1) * 128] = g * jax.nn.sigmoid(g)

    def some(i, carry):
        fetch(i).wait()

        @pl.when(i + AHEAD < STEPS)
        def _():
            fetch(i + AHEAD).start()

        for j in range(PER_STEP):
            t = i * PER_STEP + j
            for h in range(6):
                q_full = as_columns(queries[t, h : h + 1, :])
                readouts[t, h : h + 1, :] = jnp.sum(q_full * buf[t, h], axis=0, keepdims=True)
        return carry

    lax.fori_loop(0, STEPS, some, 0)
    gains = gain[...].astype(F32).reshape(1, 768)
    for h in range(6):
        at = slice(h * 128, (h + 1) * 128)
        r = readouts[:, h, :] + added[h]
        centred = r - jnp.mean(r, axis=-1, keepdims=True)
        unit = centred * lax.rsqrt(jnp.mean(centred * centred, axis=-1, keepdims=True) + EPS)
        kept = (unit * gains[:, at] * gates[:, at]).astype(BF16)
        for s in range(16):
            sent[s, :, at] = kept


def recall(parts, cosine, sine, gain, state):
    return pl.pallas_call(
        recall_body,
        in_specs=[VMEM, HBM, HBM, VMEM, HBM],
        out_specs=[VMEM] * 3,
        out_shape=[
            jax.ShapeDtypeStruct((16, 16, 768), BF16),
            jax.ShapeDtypeStruct((16, 8, 128), F32),
            jax.ShapeDtypeStruct((16, 8, 128), F32),
        ],
        scratch_shapes=[
            pltpu.VMEM((16, 6, 128, 128), F32),
            pltpu.VMEM((2, 16, 128), F32),
            pltpu.VMEM((16, 8, 128), F32),
            pltpu.VMEM((16, 768), F32),
            pltpu.VMEM((16, 8, 128), F32),
            pltpu.SemaphoreType.DMA((STEPS + 2,)),
        ],
        compiler_params=pltpu.CompilerParams(vmem_limit_bytes=57 * 2**20),
        name="recall",
    )(parts, cosine, sine, gain, state)


def renew_body(keys, values, state_ref, new_state, buf, sems):
    def fetch(i):
        return pltpu.make_async_copy(
            state_ref.at[some_rows(i)], buf.at[some_rows(i)], sems.at[i]
        )

    def store(i):
        return pltpu.make_async_copy(
            buf.at[some_rows(i)], new_state.at[some_rows(i)], sems.at[STEPS + i]
        )

    for i in range(STEPS):
        fetch(i).start()
    gamma = gammas()

    def some(i, carry):
        fetch(i).wait()
        for j in range(PER_STEP):
            t = i * PER_STEP + j
            for h in range(6):
                k_full = as_columns(keys[t, h : h + 1, :])
                buf[t, h] = gamma[h] * buf[t, h] + k_full * values[t, h : h + 1, :]
        store(i).start()
        return carry

    lax.fori_loop(0, STEPS, some, 0)
    for i in range(STEPS):
        store(i).wait()


def renew(keys, values, state):
    return pl.pallas_call(
        renew_body,
        in_specs=[VMEM, VMEM, HBM],
        out_specs=HBM,
        out_shape=jax.ShapeDtypeStruct((16, 6, 128, 128), F32),
        scratch_shapes=[
            pltpu.VMEM((16, 6, 128, 128), F32),
            pltpu.SemaphoreType.DMA((2 * STEPS,)),
        ],
        compiler_params=pltpu.CompilerParams(vmem_limit_bytes=57 * 2**20),
        name="renew",
    )(keys, values, state)


def mix_body(kept, c0, c1, c2, c3, keep, give, wide, mixed):
    xi = lax.axis_index("x")
    core = lax.axis_index("tp")
    for offset, chunk in zip(OFFSETS, (c0, c1, c2, c3)):
        at = pl.multiple_of(((xi + offset) % 4) * 32, 32)
        wide[pl.ds(at, 32), :] = chunk[...]
    rows = kept[...].reshape(256, 768)
    out = lax.dot_general(rows, wide[...], NT, preferred_element_type=F32)
    mixed[...] = out.reshape(16, 16, 128)
    keep[...] = mixed[:, pl.ds(pl.multiple_of(core * 8, 8), 8), :].astype(BF16)
    give[...] = mixed[:, pl.ds(pl.multiple_of((1 - core) * 8, 8), 8), :].astype(BF16)


def mix(kept, chunks):
    half = jax.ShapeDtypeStruct((16, 8, 128), BF16)
    return pl.pallas_call(
        mix_body,
        in_specs=[VMEM] * 5,
        out_shape=[half, half],
        scratch_shapes=[pltpu.VMEM((128, 768), BF16), pltpu.VMEM((16, 16, 128), F32)],
        compiler_params=pltpu.CompilerParams(vmem_limit_bytes=6 * 2**20),
        name="mix",
    )(kept, *chunks)


def settle_body(mine, other, got, out_ref):
    mixer_out = (mine[...].astype(F32) + other[...].astype(F32)).astype(BF16)
    res = (got[:, 16:24, :].astype(F32) + mixer_out.astype(F32)).astype(BF16).reshape(128, 128)
    for s in range(16):
        out_ref[s] = res


def settle(mine, other, got):
    return pl.pallas_call(
        settle_body,
        out_shape=jax.ShapeDtypeStruct((16, 128, 128), BF16),
        compiler_params=pltpu.CompilerParams(vmem_limit_bytes=4 * 2**20),
        name="settle",
    )(mine, other, got)


def spread_body(res, gain, branch, pick, plane, s0, s1, s2, s3, opening, own):
    total = jnp.zeros((128, 128), F32)
    for s in range(16):
        r = res[s].astype(F32)
        total = total + r * r
    scale = lax.rsqrt(jnp.sum(total, axis=-1, keepdims=True) / D + EPS)
    first = pl.multiple_of(lax.axis_index(PLANE) * 8, 8)
    gains = gain[...].astype(F32).reshape(1, D)
    branches = branch[...].astype(F32).reshape(1, D)
    dots = jnp.zeros((128, 128), F32)
    for s in range(16):
        at = slice(s * 128, (s + 1) * 128)
        n = (res[s].astype(F32) * scale * gains[:, at]).astype(BF16)
        plane[:, at] = n
        dots = dots + n.astype(F32) * branches[:, at]
        rows = jnp.dot(pick[...], n, preferred_element_type=F32).astype(BF16)
        for k, out in enumerate((s0, s1, s2, s3)):
            out[:, at] = rows[k * 32 : (k + 1) * 32]
        own[:, at] = res[s, pl.ds(first, 8), :]
    opening[...] = jax.nn.sigmoid(jnp.sum(dots, axis=-1, keepdims=True))


def spread(res, gain, branch, pick):
    rows = jax.ShapeDtypeStruct((32, D), BF16)
    return pl.pallas_call(
        spread_body,
        in_specs=[VMEM] * 4,
        out_shape=[
            jax.ShapeDtypeStruct((128, D), BF16), rows, rows, rows, rows,
            jax.ShapeDtypeStruct((128, 1), F32),
            jax.ShapeDtypeStruct((8, D), BF16),
        ],
        compiler_params=pltpu.CompilerParams(vmem_limit_bytes=10 * 2**20),
        name="spread",
    )(res, gain, branch, pick)


def dense_body(plane, c0, c1, c2, c3, hidden, down, gate, up):
    for r, chunk in enumerate((c0, c1, c2, c3)):
        for q in range(2):
            at = slice((2 * r + q) * 32, (2 * r + q + 1) * 32)
            low = q * 96
            gate[at, :] = chunk[low : low + 32, :]
            up[at, :] = chunk[low + 32 : low + 64, :]
            down[at, :] = chunk[low + 64 : low + 96, :]
    x = plane[...]
    g = lax.dot_general(x, gate[...], NT, preferred_element_type=F32)
    u = lax.dot_general(x, up[...], NT, preferred_element_type=F32)
    hidden[...] = (g * jax.nn.sigmoid(g) * u).astype(BF16)


def dense_first(plane, chunks):
    return pl.pallas_call(
        dense_body,
        out_shape=[
            jax.ShapeDtypeStruct((128, 256), BF16),
            jax.ShapeDtypeStruct((256, D), BF16),
        ],
        scratch_shapes=[pltpu.VMEM((256, D), BF16), pltpu.VMEM((256, D), BF16)],
        compiler_params=pltpu.CompilerParams(vmem_limit_bytes=12 * 2**20),
        name="dense_first",
    )(plane, *chunks)


def expert_body(
    a0, a1, a2, a3, gate_a, gate_b, up_a, up_b, down_a, down_b, r0, r1, r2, r3, rows
):
    for k, a in enumerate((a0, a1, a2, a3)):
        rows[k * 32 : (k + 1) * 32, :] = a[...]
    hidden = []
    for gate, up in ((gate_a, up_a), (gate_b, up_b)):
        g = jnp.dot(rows[...], gate[0], preferred_element_type=F32)
        u = jnp.dot(rows[...], up[0], preferred_element_type=F32)
        hidden.append((g * jax.nn.sigmoid(g) * u).astype(BF16))
    for j in range(4):
        at = slice(j * 512, (j + 1) * 512)
        out = jnp.dot(hidden[0], down_a[0, :, at], preferred_element_type=F32)
        out = (out + jnp.dot(hidden[1], down_b[0, :, at], preferred_element_type=F32)).astype(BF16)
        for k, r in enumerate((r0, r1, r2, r3)):
            r[:, at] = out[k * 32 : (k + 1) * 32, :]


def experts(arrived, weights):
    rows = jax.ShapeDtypeStruct((32, D), BF16)
    return pl.pallas_call(
        expert_body,
        in_specs=[VMEM] * 10,
        out_shape=[rows] * 4,
        scratch_shapes=[pltpu.VMEM((128, D), BF16)],
        compiler_params=pltpu.CompilerParams(vmem_limit_bytes=24 * 2**20),
        name="experts",
    )(*arrived, *weights)


def combine_body(hidden, down, opening, weigh, b0, b1, b2, b3, out, back):
    for k, b in enumerate((b0, b1, b2, b3)):
        back[k * 32 : (k + 1) * 32, :] = b[...]
        back[128 + k * 32 : 128 + (k + 1) * 32, :] = b[...]
    opened = opening[...]
    for j in range(4):
        at = slice(j * 512, (j + 1) * 512)
        term = jnp.dot(hidden[...], down[:, at], preferred_element_type=F32) * opened
        term = term + lax.dot_general(weigh[...], back[:, at], TN, preferred_element_type=F32)
        out[:, :, at] = term.astype(BF16).reshape(16, 8, 512)


def combine(hidden, down, opening, weigh, back):
    return pl.pallas_call(
        combine_body,
        out_shape=jax.ShapeDtypeStruct((16, 8, D), BF16),
        scratch_shapes=[pltpu.VMEM((256, D), BF16)],
        compiler_params=pltpu.CompilerParams(vmem_limit_bytes=12 * 2**20),
        name="combine",
    )(hidden, down, opening, weigh, *back)


def hoist_body(*refs):
    n = len(refs) // 2
    ins, outs, sems = refs[:n], refs[n : 2 * n], refs[2 * n]
    moves = [
        pltpu.make_async_copy(a.at[0, half], b.at[0, half], sems.at[2 * i + j])
        for i, (a, b) in enumerate(zip(ins, outs))
        for j, half in enumerate((pl.ds(0, a.shape[1] // 2), pl.ds(a.shape[1] // 2, a.shape[1] // 2)))
    ]
    for m in moves:
        m.start()
    for m in moves:
        m.wait()


def hoist(*arrays):
    return pl.pallas_call(
        hoist_body,
        in_specs=[HBM] * len(arrays),
        out_specs=[VMEM] * len(arrays),
        out_shape=[jax.ShapeDtypeStruct(a.shape, a.dtype) for a in arrays],
        scratch_shapes=[pltpu.SemaphoreType.DMA((2 * len(arrays),))],
        compiler_params=pltpu.CompilerParams(vmem_limit_bytes=40 * 2**20),
        name="hoist",
    )(*arrays)


def plane_exchange(array):
    return lax.all_to_all(array, PLANE, split_axis=0, concat_axis=0, tiled=True)


def routing_body(got, pick, weigh):
    total = got[0, 24:32, :].astype(F32)
    for s in range(1, 16):
        total = total + got[s, 24:32, :].astype(F32)
    ids, weights = total[0:4], total[4:8]
    share = weights / jnp.sum(weights, axis=0, keepdims=True)
    a = lax.broadcasted_iota(jnp.int32, (128, 128), 0)
    b = lax.broadcasted_iota(jnp.int32, (128, 128), 1)
    before = ((a // 8 == b // 8) & (a < b)).astype(F32).astype(BF16)
    slot = lax.broadcasted_iota(jnp.int32, (32, 128), 0)
    token = lax.broadcasted_iota(jnp.int32, (32, 128), 1)
    mine = slot // 2 == token // 8
    x_at = lax.axis_index("x")
    zy_at = lax.axis_index(PLANE)
    for k in range(4):
        wanted = (zy_at * 4 + (x_at + k) % 4).astype(F32)
        hits = (ids == wanted).astype(F32)
        match = jnp.sum(hits, axis=0, keepdims=True)
        share_of = jnp.sum(hits * share, axis=0, keepdims=True)
        many = jnp.broadcast_to(match, (32, 128))
        rank = jnp.dot(many.astype(BF16), before, preferred_element_type=F32)
        place = mine & (rank == (slot % 2).astype(F32)) & (many > 0)
        at = slice(k * 32, (k + 1) * 32)
        pick[at, :] = jnp.where(place, 1.0, 0.0).astype(BF16)
        value = jnp.where(place, jnp.broadcast_to(share_of, (32, 128)), 0.0)
        high = value.astype(BF16)
        weigh[at, :] = high
        weigh[k * 32 + 128 : k * 32 + 160, :] = (value - high.astype(F32)).astype(BF16)


def routing(got):
    return pl.pallas_call(
        routing_body,
        out_shape=[
            jax.ShapeDtypeStruct((128, 128), BF16),
            jax.ShapeDtypeStruct((256, 128), BF16),
        ],
        compiler_params=pltpu.CompilerParams(vmem_limit_bytes=4 * 2**20),
        name="routing",
    )(got)


def on_device(
    inputs, positions, ret_state, norm_mix, w_query, w_key, w_value, w_gate_in, head_gain, w_out,
    norm_ffn, route_ids, route_weight, exp_gate, exp_up, exp_down, dense_gate, dense_up, dense_down,
    branch_gate,
):
    core = lax.axis_index("tp")

    sent, w4 = prepare(
        inputs, norm_mix, route_ids.T, route_weight.T, (w_query, w_key, w_value, w_gate_in)
    )
    chunks = ring_gather(w4)
    got = plane_exchange(sent)

    partial = project(got, chunks)
    partial, positions, dense_gate, dense_up, dense_down = lax.optimization_barrier(
        (partial, positions, dense_gate, dense_up, dense_down)
    )
    angles = positions.astype(F32)[:, None] * FREQUENCY[None, :]
    cosine = jnp.cos(angles)
    sine = jnp.sin(angles) * TURN[None, :]
    dense = jnp.concatenate([dense_gate.T, dense_up.T, dense_down], axis=0)
    expert_own = (exp_gate, exp_up, exp_down)
    parts = plane_exchange(partial)

    dense_other = lax.ppermute(dense, "tp", SWAP)
    out_chunks = ring_gather(w_out.T)
    dense_chunks = ring_gather(jnp.concatenate([dense, dense_other], axis=0))
    expert_other = tuple(lax.ppermute(w, "tp", SWAP) for w in expert_own)
    kept, keys, values = recall(parts, cosine, sine, head_gain, ret_state)
    kept = plane_exchange(kept)
    pick, weigh = routing(got)
    kept, out_chunks, expert_other = lax.optimization_barrier((kept, out_chunks, expert_other))
    keep, give = mix(kept, out_chunks)
    settled = settle(keep, lax.ppermute(give, "tp", SWAP), got)
    res = plane_exchange(settled)
    res, dense_chunks = lax.optimization_barrier((res, dense_chunks))
    new_state = renew(keys, values, ret_state)

    plane, s0, s1, s2, s3, opening, own_res = spread(res, norm_ffn, branch_gate, pick)
    arrived = (
        s0,
        lax.ppermute(s1, "x", RIGHT),
        lax.ppermute(s2, "x", ACROSS),
        lax.ppermute(s3, "x", LEFT),
    )
    hidden, down = dense_first(plane, dense_chunks)
    weights = tuple(w for pair in zip(expert_own, expert_other) for w in pair)
    weights = hoist(*weights)
    r0, r1, r2, r3 = experts(arrived, weights)
    back = (
        r0,
        lax.ppermute(r1, "x", LEFT),
        lax.ppermute(r2, "x", ACROSS),
        lax.ppermute(r3, "x", RIGHT),
    )
    branch = combine(hidden, down, opening, weigh, back)
    terms = plane_exchange(branch)
    summed = jnp.sum(terms.astype(F32), axis=0)
    mine = (own_res.astype(F32) + summed).astype(BF16)
    other = lax.ppermute(mine, "tp", SWAP)
    layer_out = jnp.concatenate(
        [jnp.where(core == 0, mine, other), jnp.where(core == 0, other, mine)], axis=0
    )
    return (layer_out, new_state)


EP = ("z", "y", "x")


def solution(mesh):
    inner = Mesh(mesh.devices.reshape(4, 4, 4, 2), ("z", "y", "x", "tp"))
    in_specs = (
        P(EP, None),
        P(EP),
        P(EP, "tp", None, None),
        P(),
        P(EP, "tp"),
        P(EP, "tp"),
        P(EP, "tp"),
        P(EP, "tp"),
        P("tp"),
        P("tp", EP),
        P(),
        P(EP, None),
        P(EP, None),
        P(EP, None, "tp"),
        P(EP, None, "tp"),
        P(EP, "tp", None),
        P(None, (*EP, "tp")),
        P(None, (*EP, "tp")),
        P((*EP, "tp"), None),
        P(),
    )
    out_specs = (P(EP, None), P(EP, "tp", None, None))
    return jax.shard_map(
        on_device, mesh=inner, in_specs=in_specs, out_specs=out_specs, check_vma=False
    )
```

```python
import jax
import jax.numpy as jnp
import numpy as np
from jax import lax
from jax.experimental import pallas as pl
from jax.experimental.pallas import tpu as pltpu
from jax.sharding import Mesh, PartitionSpec as P


D = 2048
HEADS = 12
EPS = 1e-06
F32 = jnp.float32
BF16 = jnp.bfloat16

RIGHT = [(i, (i + 1) % 4) for i in range(4)]
LEFT = [(i, (i - 1) % 4) for i in range(4)]
ACROSS = [(i, (i + 2) % 4) for i in range(4)]
SWAP = [(0, 1), (1, 0)]
PLANE = ("z", "y")
NT = (((1,), (1,)), ((), ()))
TN = (((0,), (0,)), ((), ()))
HBM = pl.BlockSpec(memory_space=pltpu.HBM)
VMEM = pl.BlockSpec(memory_space=pltpu.VMEM)


def ring_gather(own):
    return (
        own,
        lax.ppermute(own, "x", RIGHT),
        lax.ppermute(own, "x", ACROSS),
        lax.ppermute(own, "x", LEFT),
    )


OFFSETS = (0, 3, 2, 1)


SMEM = pl.BlockSpec(memory_space=pltpu.SMEM)


def prepare_body(x_ref, gain, ids, shares, wq, wk, wv, wg, sent, w4, routes):
    w4[0] = wq[...]
    w4[1] = wk[...]
    w4[2] = wv[...]
    w4[3] = wg[...]
    half = x_ref[pl.ds(pl.multiple_of(lax.axis_index("tp") * 8, 8), 8), :]
    routes[...] = jnp.zeros((8, 128), F32)
    routes[0:4, 0:16] = ids[...].astype(F32)
    routes[4:8, 0:16] = shares[...].astype(F32)
    first = lax.axis_index(PLANE) * 8
    turned = pltpu.roll(routes[...], (first - lax.axis_index("tp") * 8 + 128) % 128, 1)
    lane = lax.broadcasted_iota(jnp.int32, (8, 128), 1)
    route = jnp.where(lane // 8 == first // 8, turned, 0.0).astype(BF16)
    x = x_ref[...]
    v = x.astype(F32)
    scaled = v * lax.rsqrt(jnp.mean(v * v, axis=-1, keepdims=True) + EPS)
    normed = (scaled * gain[...].astype(F32).reshape(1, D)).astype(BF16)
    for j in range(16):
        at = slice(j * 128, (j + 1) * 128)
        sent[j, 0:16, :] = normed[:, at]
        sent[j, 16:24, :] = half[:, at]
        sent[j, 24:32, :] = route


def prepare(x, gain, ids, shares, ws):
    return pl.pallas_call(
        prepare_body,
        out_shape=[
            jax.ShapeDtypeStruct((16, 32, 128), BF16),
            jax.ShapeDtypeStruct((4, 32, 768), BF16),
        ],
        scratch_shapes=[pltpu.VMEM((8, 128), F32)],
        name="prepare",
    )(x, gain, ids, shares, *ws)


def project_body(x_ref, c0, c1, c2, c3, out_ref, wide, out, sems):
    xi = lax.axis_index("x")
    x = x_ref[:, 0:16, :].reshape(256, 128)
    stores = []
    for p in range(4):
        for offset, chunk in zip(OFFSETS, (c0, c1, c2, c3)):
            at = pl.multiple_of(((xi + offset) % 4) * 32, 32)
            wide[p, pl.ds(at, 32), :] = chunk[p]
        at = pl.ds(p * 768, 768)
        out[:, :, at] = (
            jnp.dot(x, wide[p], preferred_element_type=F32).astype(BF16).reshape(16, 16, 768)
        )
        stores.append(pltpu.make_async_copy(out.at[:, :, at], out_ref.at[:, :, at], sems.at[p]))
        stores[-1].start()
    for store in stores:
        store.wait()


def project(got, chunks):
    return pl.pallas_call(
        project_body,
        in_specs=[VMEM] * 5,
        out_specs=HBM,
        out_shape=jax.ShapeDtypeStruct((16, 16, 3072), BF16),
        scratch_shapes=[
            pltpu.VMEM((4, 128, 768), BF16),
            pltpu.VMEM((16, 16, 3072), BF16),
            pltpu.SemaphoreType.DMA((4,)),
        ],
        compiler_params=pltpu.CompilerParams(vmem_limit_bytes=12 * 2**20),
        name="project",
    )(got, *chunks)


PER_STEP = 4
STEPS = 16 // PER_STEP
AHEAD = 4
FREQUENCY = np.tile(10000.0 ** (-np.arange(64) * 2.0 / 128), 2).astype(np.float32)
TURN = np.repeat([-1.0, 1.0], 64).astype(np.float32)
GAMMA = [float(np.exp(np.log1p(-(2.0 ** (-5.0 - 5.0 * h / (HEADS - 1)))))) for h in range(HEADS)]


def gammas():
    upper = lax.axis_index("tp") == 1
    return [jnp.where(upper, GAMMA[h + 6], GAMMA[h]).astype(F32) for h in range(6)]


def as_columns(row):
    return jnp.transpose(jnp.broadcast_to(row, (128, 128)))


def some_rows(i):
    return pl.ds(i * PER_STEP, PER_STEP)


def recall_body(
    parts, cosine_ref, sine_ref, gain, state_ref, sent, keys, values,
    buf, turns, queries, gates, readouts, sems,
):
    fetch_turns = [
        pltpu.make_async_copy(cosine_ref, turns.at[0], sems.at[STEPS]),
        pltpu.make_async_copy(sine_ref, turns.at[1], sems.at[STEPS + 1]),
    ]
    for c in fetch_turns:
        c.start()

    def fetch(i):
        return pltpu.make_async_copy(
            state_ref.at[some_rows(i)], buf.at[some_rows(i)], sems.at[i]
        )

    for i in range(AHEAD):
        fetch(i).start()
    gamma = gammas()
    for c in fetch_turns:
        c.wait()
    cos_v, sin_v = turns[0], turns[1]
    keys[...] = jnp.zeros((16, 8, 128), F32)
    values[...] = jnp.zeros((16, 8, 128), F32)
    added = []
    for h in range(6):
        def total(which):
            at = which * 768 + h * 128
            acc = parts[0, :, at : at + 128].astype(F32)
            for s in range(1, 16):
                acc = acc + parts[s, :, at : at + 128].astype(F32)
            return acc.astype(BF16).astype(F32)

        q, k, v, g = (total(i) for i in range(4))
        query = q * cos_v + pltpu.roll(q, 64, 1) * sin_v
        key = (k * cos_v + pltpu.roll(k, 64, 1) * sin_v) * (128.0 ** -0.5)
        queries[:, h, :] = gamma[h] * query
        keys[:, h, :] = key
        values[:, h, :] = v
        added.append(jnp.sum(query * key, axis=-1, keepdims=True) * v)
        gates[:, h * 128 : (h + 1) * 128] = g * jax.nn.sigmoid(g)

    def some(i, carry):
        fetch(i).wait()

        @pl.when(i + AHEAD < STEPS)
        def _():
            fetch(i + AHEAD).start()

        for j in range(PER_STEP):
            t = i * PER_STEP + j
            for h in range(6):
                q_full = as_columns(queries[t, h : h + 1, :])
                readouts[t, h : h + 1, :] = jnp.sum(q_full * buf[t, h], axis=0, keepdims=True)
        return carry

    lax.fori_loop(0, STEPS, some, 0)
    gains = gain[...].astype(F32).reshape(1, 768)
    for h in range(6):
        at = slice(h * 128, (h + 1) * 128)
        r = readouts[:, h, :] + added[h]
        centred = r - jnp.mean(r, axis=-1, keepdims=True)
        unit = centred * lax.rsqrt(jnp.mean(centred * centred, axis=-1, keepdims=True) + EPS)
        kept = (unit * gains[:, at] * gates[:, at]).astype(BF16)
        for s in range(16):
            sent[s, :, at] = kept


def recall(parts, cosine, sine, gain, state):
    return pl.pallas_call(
        recall_body,
        in_specs=[VMEM, HBM, HBM, VMEM, HBM],
        out_specs=[VMEM] * 3,
        out_shape=[
            jax.ShapeDtypeStruct((16, 16, 768), BF16),
            jax.ShapeDtypeStruct((16, 8, 128), F32),
            jax.ShapeDtypeStruct((16, 8, 128), F32),
        ],
        scratch_shapes=[
            pltpu.VMEM((16, 6, 128, 128), F32),
            pltpu.VMEM((2, 16, 128), F32),
            pltpu.VMEM((16, 8, 128), F32),
            pltpu.VMEM((16, 768), F32),
            pltpu.VMEM((16, 8, 128), F32),
            pltpu.SemaphoreType.DMA((STEPS + 2,)),
        ],
        compiler_params=pltpu.CompilerParams(vmem_limit_bytes=57 * 2**20),
        name="recall",
    )(parts, cosine, sine, gain, state)


def renew_body(keys, values, state_ref, new_state, buf, sems):
    def fetch(i):
        return pltpu.make_async_copy(
            state_ref.at[some_rows(i)], buf.at[some_rows(i)], sems.at[i]
        )

    def store(i):
        return pltpu.make_async_copy(
            buf.at[some_rows(i)], new_state.at[some_rows(i)], sems.at[STEPS + i]
        )

    for i in range(STEPS):
        fetch(i).start()
    gamma = gammas()

    def some(i, carry):
        fetch(i).wait()
        for j in range(PER_STEP):
            t = i * PER_STEP + j
            for h in range(6):
                k_full = as_columns(keys[t, h : h + 1, :])
                buf[t, h] = gamma[h] * buf[t, h] + k_full * values[t, h : h + 1, :]
        store(i).start()
        return carry

    lax.fori_loop(0, STEPS, some, 0)
    for i in range(STEPS):
        store(i).wait()


def renew(keys, values, state):
    return pl.pallas_call(
        renew_body,
        in_specs=[VMEM, VMEM, HBM],
        out_specs=HBM,
        out_shape=jax.ShapeDtypeStruct((16, 6, 128, 128), F32),
        scratch_shapes=[
            pltpu.VMEM((16, 6, 128, 128), F32),
            pltpu.SemaphoreType.DMA((2 * STEPS,)),
        ],
        compiler_params=pltpu.CompilerParams(vmem_limit_bytes=57 * 2**20),
        name="renew",
    )(keys, values, state)


def mix_body(kept, c0, c1, c2, c3, keep, give, wide, mixed):
    xi = lax.axis_index("x")
    core = lax.axis_index("tp")
    for offset, chunk in zip(OFFSETS, (c0, c1, c2, c3)):
        at = pl.multiple_of(((xi + offset) % 4) * 32, 32)
        wide[pl.ds(at, 32), :] = chunk[...]
    rows = kept[...].reshape(256, 768)
    out = lax.dot_general(rows, wide[...], NT, preferred_element_type=F32)
    mixed[...] = out.reshape(16, 16, 128)
    keep[...] = mixed[:, pl.ds(pl.multiple_of(core * 8, 8), 8), :].astype(BF16)
    give[...] = mixed[:, pl.ds(pl.multiple_of((1 - core) * 8, 8), 8), :].astype(BF16)


def mix(kept, chunks):
    half = jax.ShapeDtypeStruct((16, 8, 128), BF16)
    return pl.pallas_call(
        mix_body,
        in_specs=[VMEM] * 5,
        out_shape=[half, half],
        scratch_shapes=[pltpu.VMEM((128, 768), BF16), pltpu.VMEM((16, 16, 128), F32)],
        compiler_params=pltpu.CompilerParams(vmem_limit_bytes=6 * 2**20),
        name="mix",
    )(kept, *chunks)


def settle_body(mine, other, got, out_ref):
    mixer_out = (mine[...].astype(F32) + other[...].astype(F32)).astype(BF16)
    res = (got[:, 16:24, :].astype(F32) + mixer_out.astype(F32)).astype(BF16).reshape(128, 128)
    for s in range(16):
        out_ref[s] = res


def settle(mine, other, got):
    return pl.pallas_call(
        settle_body,
        out_shape=jax.ShapeDtypeStruct((16, 128, 128), BF16),
        compiler_params=pltpu.CompilerParams(vmem_limit_bytes=4 * 2**20),
        name="settle",
    )(mine, other, got)


def spread_body(res, gain, branch, pick, plane, s0, s1, s2, s3, opening, own):
    total = jnp.zeros((128, 128), F32)
    for s in range(16):
        r = res[s].astype(F32)
        total = total + r * r
    scale = lax.rsqrt(jnp.sum(total, axis=-1, keepdims=True) / D + EPS)
    first = pl.multiple_of(lax.axis_index(PLANE) * 8, 8)
    gains = gain[...].astype(F32).reshape(1, D)
    branches = branch[...].astype(F32).reshape(1, D)
    dots = jnp.zeros((128, 128), F32)
    for s in range(16):
        at = slice(s * 128, (s + 1) * 128)
        n = (res[s].astype(F32) * scale * gains[:, at]).astype(BF16)
        plane[:, at] = n
        dots = dots + n.astype(F32) * branches[:, at]
        rows = jnp.dot(pick[...], n, preferred_element_type=F32).astype(BF16)
        for k, out in enumerate((s0, s1, s2, s3)):
            out[:, at] = rows[k * 32 : (k + 1) * 32]
        own[:, at] = res[s, pl.ds(first, 8), :]
    opening[...] = jax.nn.sigmoid(jnp.sum(dots, axis=-1, keepdims=True))


def spread(res, gain, branch, pick):
    rows = jax.ShapeDtypeStruct((32, D), BF16)
    return pl.pallas_call(
        spread_body,
        in_specs=[VMEM] * 4,
        out_shape=[
            jax.ShapeDtypeStruct((128, D), BF16), rows, rows, rows, rows,
            jax.ShapeDtypeStruct((128, 1), F32),
            jax.ShapeDtypeStruct((8, D), BF16),
        ],
        compiler_params=pltpu.CompilerParams(vmem_limit_bytes=10 * 2**20),
        name="spread",
    )(res, gain, branch, pick)


def dense_body(plane, c0, c1, c2, c3, hidden, down, gate, up):
    for r, chunk in enumerate((c0, c1, c2, c3)):
        for q in range(2):
            at = slice((2 * r + q) * 32, (2 * r + q + 1) * 32)
            low = q * 96
            gate[at, :] = chunk[low : low + 32, :]
            up[at, :] = chunk[low + 32 : low + 64, :]
            down[at, :] = chunk[low + 64 : low + 96, :]
    x = plane[...]
    g = lax.dot_general(x, gate[...], NT, preferred_element_type=F32)
    u = lax.dot_general(x, up[...], NT, preferred_element_type=F32)
    hidden[...] = (g * jax.nn.sigmoid(g) * u).astype(BF16)


def dense_first(plane, chunks):
    return pl.pallas_call(
        dense_body,
        out_shape=[
            jax.ShapeDtypeStruct((128, 256), BF16),
            jax.ShapeDtypeStruct((256, D), BF16),
        ],
        scratch_shapes=[pltpu.VMEM((256, D), BF16), pltpu.VMEM((256, D), BF16)],
        compiler_params=pltpu.CompilerParams(vmem_limit_bytes=12 * 2**20),
        name="dense_first",
    )(plane, *chunks)


def expert_body(
    a0, a1, a2, a3, gate_a, gate_b, up_a, up_b, down_a, down_b, r0, r1, r2, r3, rows
):
    for k, a in enumerate((a0, a1, a2, a3)):
        rows[k * 32 : (k + 1) * 32, :] = a[...]
    hidden = []
    for gate, up in ((gate_a, up_a), (gate_b, up_b)):
        g = jnp.dot(rows[...], gate[0], preferred_element_type=F32)
        u = jnp.dot(rows[...], up[0], preferred_element_type=F32)
        hidden.append((g * jax.nn.sigmoid(g) * u).astype(BF16))
    for j in range(4):
        at = slice(j * 512, (j + 1) * 512)
        out = jnp.dot(hidden[0], down_a[0, :, at], preferred_element_type=F32)
        out = (out + jnp.dot(hidden[1], down_b[0, :, at], preferred_element_type=F32)).astype(BF16)
        for k, r in enumerate((r0, r1, r2, r3)):
            r[:, at] = out[k * 32 : (k + 1) * 32, :]


def experts(arrived, weights):
    rows = jax.ShapeDtypeStruct((32, D), BF16)
    return pl.pallas_call(
        expert_body,
        in_specs=[VMEM] * 10,
        out_shape=[rows] * 4,
        scratch_shapes=[pltpu.VMEM((128, D), BF16)],
        compiler_params=pltpu.CompilerParams(vmem_limit_bytes=24 * 2**20),
        name="experts",
    )(*arrived, *weights)


def combine_body(hidden, down, opening, weigh, b0, b1, b2, b3, out, back):
    for k, b in enumerate((b0, b1, b2, b3)):
        back[k * 32 : (k + 1) * 32, :] = b[...]
        back[128 + k * 32 : 128 + (k + 1) * 32, :] = b[...]
    opened = opening[...]
    for j in range(4):
        at = slice(j * 512, (j + 1) * 512)
        term = jnp.dot(hidden[...], down[:, at], preferred_element_type=F32) * opened
        term = term + lax.dot_general(weigh[...], back[:, at], TN, preferred_element_type=F32)
        out[:, :, at] = term.astype(BF16).reshape(16, 8, 512)


def combine(hidden, down, opening, weigh, back):
    return pl.pallas_call(
        combine_body,
        out_shape=jax.ShapeDtypeStruct((16, 8, D), BF16),
        scratch_shapes=[pltpu.VMEM((256, D), BF16)],
        compiler_params=pltpu.CompilerParams(vmem_limit_bytes=12 * 2**20),
        name="combine",
    )(hidden, down, opening, weigh, *back)


def hoist_body(*refs):
    n = len(refs) // 2
    ins, outs, sems = refs[:n], refs[n : 2 * n], refs[2 * n]
    moves = [
        pltpu.make_async_copy(a, b, sems.at[i]) for i, (a, b) in enumerate(zip(ins, outs))
    ]
    for m in moves:
        m.start()
    for m in moves:
        m.wait()


def hoist(*arrays):
    return pl.pallas_call(
        hoist_body,
        in_specs=[HBM] * len(arrays),
        out_specs=[VMEM] * len(arrays),
        out_shape=[jax.ShapeDtypeStruct(a.shape, a.dtype) for a in arrays],
        scratch_shapes=[pltpu.SemaphoreType.DMA((len(arrays),))],
        compiler_params=pltpu.CompilerParams(vmem_limit_bytes=40 * 2**20),
        name="hoist",
    )(*arrays)


def plane_exchange(array):
    return lax.all_to_all(array, PLANE, split_axis=0, concat_axis=0, tiled=True)


def routing_body(got, pick, weigh):
    total = got[0, 24:32, :].astype(F32)
    for s in range(1, 16):
        total = total + got[s, 24:32, :].astype(F32)
    ids, weights = total[0:4], total[4:8]
    share = weights / jnp.sum(weights, axis=0, keepdims=True)
    a = lax.broadcasted_iota(jnp.int32, (128, 128), 0)
    b = lax.broadcasted_iota(jnp.int32, (128, 128), 1)
    before = ((a // 8 == b // 8) & (a < b)).astype(F32).astype(BF16)
    slot = lax.broadcasted_iota(jnp.int32, (32, 128), 0)
    token = lax.broadcasted_iota(jnp.int32, (32, 128), 1)
    mine = slot // 2 == token // 8
    x_at = lax.axis_index("x")
    zy_at = lax.axis_index(PLANE)
    for k in range(4):
        wanted = (zy_at * 4 + (x_at + k) % 4).astype(F32)
        hits = (ids == wanted).astype(F32)
        match = jnp.sum(hits, axis=0, keepdims=True)
        share_of = jnp.sum(hits * share, axis=0, keepdims=True)
        many = jnp.broadcast_to(match, (32, 128))
        rank = jnp.dot(many.astype(BF16), before, preferred_element_type=F32)
        place = mine & (rank == (slot % 2).astype(F32)) & (many > 0)
        at = slice(k * 32, (k + 1) * 32)
        pick[at, :] = jnp.where(place, 1.0, 0.0).astype(BF16)
        value = jnp.where(place, jnp.broadcast_to(share_of, (32, 128)), 0.0)
        high = value.astype(BF16)
        weigh[at, :] = high
        weigh[k * 32 + 128 : k * 32 + 160, :] = (value - high.astype(F32)).astype(BF16)


def routing(got):
    return pl.pallas_call(
        routing_body,
        out_shape=[
            jax.ShapeDtypeStruct((128, 128), BF16),
            jax.ShapeDtypeStruct((256, 128), BF16),
        ],
        compiler_params=pltpu.CompilerParams(vmem_limit_bytes=4 * 2**20),
        name="routing",
    )(got)


def on_device(
    inputs, positions, ret_state, norm_mix, w_query, w_key, w_value, w_gate_in, head_gain, w_out,
    norm_ffn, route_ids, route_weight, exp_gate, exp_up, exp_down, dense_gate, dense_up, dense_down,
    branch_gate,
):
    core = lax.axis_index("tp")

    sent, w4 = prepare(
        inputs, norm_mix, route_ids.T, route_weight.T, (w_query, w_key, w_value, w_gate_in)
    )
    chunks = ring_gather(w4)
    got = plane_exchange(sent)

    partial = project(got, chunks)
    partial, positions, dense_gate, dense_up, dense_down = lax.optimization_barrier(
        (partial, positions, dense_gate, dense_up, dense_down)
    )
    angles = positions.astype(F32)[:, None] * FREQUENCY[None, :]
    cosine = jnp.cos(angles)
    sine = jnp.sin(angles) * TURN[None, :]
    dense = jnp.concatenate([dense_gate.T, dense_up.T, dense_down], axis=0)
    expert_own = (exp_gate, exp_up, exp_down)
    parts = plane_exchange(partial)

    dense_other = lax.ppermute(dense, "tp", SWAP)
    out_chunks = ring_gather(w_out.T)
    dense_chunks = ring_gather(jnp.concatenate([dense, dense_other], axis=0))
    expert_other = tuple(lax.ppermute(w, "tp", SWAP) for w in expert_own)
    kept, keys, values = recall(parts, cosine, sine, head_gain, ret_state)
    kept = plane_exchange(kept)
    pick, weigh = routing(got)
    kept, out_chunks, expert_other = lax.optimization_barrier((kept, out_chunks, expert_other))
    keep, give = mix(kept, out_chunks)
    settled = settle(keep, lax.ppermute(give, "tp", SWAP), got)
    res = plane_exchange(settled)
    res, dense_chunks = lax.optimization_barrier((res, dense_chunks))
    new_state = renew(keys, values, ret_state)

    plane, s0, s1, s2, s3, opening, own_res = spread(res, norm_ffn, branch_gate, pick)
    arrived = (
        s0,
        lax.ppermute(s1, "x", RIGHT),
        lax.ppermute(s2, "x", ACROSS),
        lax.ppermute(s3, "x", LEFT),
    )
    hidden, down = dense_first(plane, dense_chunks)
    weights = tuple(w for pair in zip(expert_own, expert_other) for w in pair)
    weights = hoist(*weights)
    r0, r1, r2, r3 = experts(arrived, weights)
    back = (
        r0,
        lax.ppermute(r1, "x", LEFT),
        lax.ppermute(r2, "x", ACROSS),
        lax.ppermute(r3, "x", RIGHT),
    )
    branch = combine(hidden, down, opening, weigh, back)
    terms = plane_exchange(branch)
    summed = jnp.sum(terms.astype(F32), axis=0)
    mine = (own_res.astype(F32) + summed).astype(BF16)
    other = lax.ppermute(mine, "tp", SWAP)
    layer_out = jnp.concatenate(
        [jnp.where(core == 0, mine, other), jnp.where(core == 0, other, mine)], axis=0
    )
    return (layer_out, new_state)


EP = ("z", "y", "x")


def solution(mesh):
    inner = Mesh(mesh.devices.reshape(4, 4, 4, 2), ("z", "y", "x", "tp"))
    in_specs = (
        P(EP, None),
        P(EP),
        P(EP, "tp", None, None),
        P(),
        P(EP, "tp"),
        P(EP, "tp"),
        P(EP, "tp"),
        P(EP, "tp"),
        P("tp"),
        P("tp", EP),
        P(),
        P(EP, None),
        P(EP, None),
        P(EP, None, "tp"),
        P(EP, None, "tp"),
        P(EP, "tp", None),
        P(None, (*EP, "tp")),
        P(None, (*EP, "tp")),
        P((*EP, "tp"), None),
        P(),
    )
    out_specs = (P(EP, None), P(EP, "tp", None, None))
    return jax.shard_map(
        on_device, mesh=inner, in_specs=in_specs, out_specs=out_specs, check_vma=False
    )
```
